32 devices in a mesh: sp: 8 (over z, x), tp: 4 (over y, core).
Axes of the slice: x: 2, y: 2, z: 4, core: 2. Of those that a mesh axis runs over, the one named last changes fastest.
Arguments:
- tokens: bfloat16 [8192, 2048], P('sp', 'tp'), may hold values from -6 to 6
- norm_gain: float32 [2048], replicated, may hold values from 0.1 to 1.9
- att_query: bfloat16 [2048, 1024], P(None, 'tp'), may hold values from -1 to 1, as said below
- att_key: bfloat16 [2048, 512], P(None, 'tp'), may hold values from -16 to 16, as said below
- att_value: bfloat16 [2048, 512], P(None, 'tp'), may hold values from -0.125 to 0.125
- ret_query: bfloat16 [2048, 512], P(None, 'tp'), may hold values from -0.125 to 0.125
- ret_key: bfloat16 [2048, 512], P(None, 'tp'), may hold values from -0.125 to 0.125
- ret_value: bfloat16 [2048, 1024], P(None, 'tp'), may hold values from -0.125 to 0.125
- ret_gate: bfloat16 [2048, 1024], P(None, 'tp'), may hold values from -0.125 to 0.125
- att_sink: float32 [16], P('tp'), may hold values from 4 to 7
- decay_log: float32 [8, 8192], P('tp', 'sp'), may hold values from -2 to 0, as said below
- init_state: float32 [2, 8, 64, 128], P(None, 'tp'), may hold values from -24 to 24
- out_att: bfloat16 [1024, 2048], P('tp'), may hold values from -0.125 to 0.125
- out_ret: bfloat16 [1024, 2048], P('tp'), may hold values from -0.125 to 0.125
Outputs:
- mixed: bfloat16 [8192, 2048], P('sp', 'tp')
The draws below stay inside these ranges and needn't reach their ends.
Inputs may be any that keep to these rules, and one draw needn't show every extreme that they name: `att_query`: entries of order D ** -0.5. `att_key`: entries of order D ** -0.5 or larger. `decay_log`: log decays, negative.
All inputs are finite; a program needn't handle non-finite values.
Results may differ from the reference program's by a relative error of at most 0.02.
Values may be sent and summed in bfloat16 or wider, within the bound.
No kernel may reach another device: no remote copies, remote signals or barrier semaphores. Data moves between devices by JAX's collectives and lax.ppermute only.
A program may use at most 64 MiB of HBM per device.

```python
import math
import jax
import jax.numpy as jnp
from jax import lax

D = 2048
ATT_HEADS = 16
KV_HEADS = 8
HD = 64
RET_HEADS = 8
RK = 64
RV = 128
WINDOW = 128
RET_BLOCK = 128
TOK_DEV = 1024
SEQUENCE_LENGTH = 8192
N_TP = 4


def draw_tokens(key, part):
    base_rows = jnp.clip(jax.random.normal(key, (SEQUENCE_LENGTH, D), jnp.float32), -6.0, 6.0)
    return base_rows.astype(jnp.bfloat16)


def attention_weights(key):
    query_w = jnp.clip(jax.random.normal(jax.random.fold_in(key, 11), (D, ATT_HEADS * HD), jnp.float32), -4.0, 4.0) * D ** (-0.5)
    key_w = jnp.clip(jax.random.normal(jax.random.fold_in(key, 12), (D, KV_HEADS * HD), jnp.float32), -4.0, 4.0) * D ** (-0.5)
    return (query_w, key_w)


def draw_att_query(key, part):
    return attention_weights(key)[0].astype(jnp.bfloat16)


def draw_att_key(key, part):
    return attention_weights(key)[1].astype(jnp.bfloat16)


def draw_decay_log(key, part):
    child_random_keys = jax.random.split(key, 7)
    slow_heads = jax.random.uniform(child_random_keys[0], (RET_HEADS,)) < 0.5
    slow_rate = 0.15 * math.log(10.0) / SEQUENCE_LENGTH * jax.random.uniform(child_random_keys[1], (RET_HEADS,), minval=0.5, maxval=1.5)
    fast_rate = jax.random.uniform(child_random_keys[2], (RET_HEADS,), minval=1.0 / 100.0, maxval=1.0 / 30.0)
    baseline_rate = jnp.where(slow_heads, slow_rate, fast_rate)
    device_pace = jnp.exp(jax.random.uniform(child_random_keys[3], (SEQUENCE_LENGTH // TOK_DEV,), minval=math.log(0.5), maxval=math.log(2.0)))
    full_speed = jnp.repeat(device_pace, TOK_DEV, total_repeat_length=SEQUENCE_LENGTH)
    jaggedness = jax.random.uniform(child_random_keys[4], (RET_HEADS, SEQUENCE_LENGTH), minval=0.5, maxval=1.5)
    spike_positions = jax.random.randint(child_random_keys[5], (3,), 0, SEQUENCE_LENGTH)
    spike_depth = jax.random.uniform(child_random_keys[6], (3,), minval=0.55, maxval=0.85)
    spike_count = jnp.zeros((SEQUENCE_LENGTH,), jnp.float32).at[spike_positions].add(jnp.log(spike_depth))
    return -baseline_rate[:, None] * full_speed[None, :] * jaggedness + spike_count[None, :]


def block_scale(rng, dims, pieces, smallest, largest):
    def one(position, shards_of):
        heights = jax.random.uniform(jax.random.fold_in(jax.random.fold_in(rng, 6), position), (shards_of,), jnp.float32, smallest / len(pieces), largest / len(pieces))
        return jnp.repeat(jnp.exp(heights), dims[position] // shards_of).reshape((-1,) + (1,) * (len(dims) - position - 1))

    loudness = one(*pieces[0])
    for cut in pieces[1:]:
        loudness = loudness * one(*cut)
    return loudness


def scatter_about(own_key, extent, scale, limit, cuts=(), held_as=jnp.bfloat16):
    result = jax.random.normal(own_key, extent, jnp.float32) * scale
    if len(cuts) > 0:
        result = block_scale(own_key, extent, cuts, -0.22, 0.18) * result
    return jnp.clip(result, min=-limit, max=limit).astype(held_as)


def setup_inputs(seed: int = 0) -> dict:
    seeds = jax.random.split(jax.random.key(seed), 15)
    tokens = draw_tokens(jax.random.fold_in(seeds[14], 71), 0)
    norm_gain = jnp.clip(1.0 + 0.18 * jax.random.normal(seeds[1], (D,), jnp.float32), 0.1, 1.9)
    att_query = draw_att_query(jax.random.fold_in(seeds[14], 71), 0)
    att_key = draw_att_key(jax.random.fold_in(seeds[14], 71), 0)
    att_value = scatter_about(seeds[4], (D, KV_HEADS * HD), D ** -0.5, 0.125, ((1, 4),))
    ret_query = scatter_about(seeds[5], (D, RET_HEADS * RK), D ** -0.5, 0.125, ((1, 4),))
    ret_key = scatter_about(seeds[6], (D, RET_HEADS * RK), D ** -0.5, 0.125, ((1, 4),))
    ret_value = scatter_about(seeds[7], (D, RET_HEADS * RV), D ** -0.5, 0.125, ((1, 4),))
    ret_gate = scatter_about(seeds[8], (D, RET_HEADS * RV), D ** -0.5, 0.125, ((1, 4),))
    att_sink = jnp.clip(4.0 + 3.0 * jax.random.uniform(seeds[9], (ATT_HEADS,), jnp.float32) ** block_scale(seeds[9], (ATT_HEADS,), ((0, 4),), -0.2, 0.2), 4.0, 7.0)
    decay_log = draw_decay_log(jax.random.fold_in(seeds[14], 71), 0)
    init_state = scatter_about(seeds[11], (2, RET_HEADS, RK, RV), 4.0, 24.0, ((1, 4),), jnp.float32)
    out_att = scatter_about(seeds[12], (ATT_HEADS * HD, D), (ATT_HEADS * HD + RET_HEADS * RV) ** -0.5, 0.125, ((0, 4),))
    out_ret = scatter_about(seeds[13], (RET_HEADS * RV, D), (ATT_HEADS * HD + RET_HEADS * RV) ** -0.5, 0.125, ((0, 4),))
    return dict(tokens=tokens, norm_gain=norm_gain, att_query=att_query, att_key=att_key, att_value=att_value, ret_query=ret_query, ret_key=ret_key, ret_value=ret_value, ret_gate=ret_gate, att_sink=att_sink, decay_log=decay_log, init_state=init_state, out_att=out_att, out_ret=out_ret)


NORM_EPS = 1e-06
ROPE_BASE = 10000.0
HIGHEST = lax.Precision.HIGHEST

def rotated(values, positions):
    half_dim = values.shape[-1] // 2
    inverse = ROPE_BASE ** (-2.0 * jnp.arange(half_dim, dtype=jnp.float32) / values.shape[-1])
    angles = positions.astype(jnp.float32)[:, None] * inverse[None, :]
    cosine = jnp.cos(angles)[:, None, :]
    sine = jnp.sin(angles)[:, None, :]
    first_half = values[..., :half_dim]
    second_half = values[..., half_dim:]
    return jnp.concatenate([first_half * cosine - second_half * sine, first_half * sine + second_half * cosine], axis=-1)

def attend_all(queries, key_proj, value_proj, att_sink):
    seq_len = queries.shape[0]
    block_rows = 512
    groups = ATT_HEADS // KV_HEADS
    span_rows = block_rows + 2 * WINDOW
    padded_keys = jnp.pad(key_proj, ((WINDOW, WINDOW), (0, 0)))
    padded_vals = jnp.pad(value_proj, ((WINDOW, WINDOW), (0, 0)))
    sink_col = att_sink.astype(jnp.float32).reshape(KV_HEADS, groups, 1, 1)

    def one_block(block_index):
        first_row = block_index * block_rows
        query_block = lax.dynamic_slice_in_dim(queries, first_row, block_rows, 0).reshape(block_rows, KV_HEADS, groups, HD)
        key_block = lax.dynamic_slice_in_dim(padded_keys, first_row, span_rows, 0).reshape(span_rows, KV_HEADS, HD)
        value_block = lax.dynamic_slice_in_dim(padded_vals, first_row, span_rows, 0).reshape(span_rows, KV_HEADS, HD)
        scores = jnp.einsum('qkgd,skd->kgqs', query_block.astype(jnp.float32), key_block.astype(jnp.float32)) * HD ** (-0.5)
        query_pos = first_row + jnp.arange(block_rows, dtype=jnp.int32)
        key_pos = first_row - WINDOW + jnp.arange(span_rows, dtype=jnp.int32)
        allowed = (jnp.abs(query_pos[:, None] - key_pos[None, :]) <= WINDOW) & (key_pos >= 0)[None, :] & (key_pos < seq_len)[None, :]
        scores = jnp.where(allowed, scores, -jnp.inf)
        row_top = jnp.maximum(lax.optimization_barrier(jnp.max(scores, axis=-1, keepdims=True)), sink_col)
        raised = jnp.exp(scores - row_top)
        denominator = lax.optimization_barrier(jnp.sum(raised, axis=-1, keepdims=True)) + jnp.exp(sink_col - row_top)
        weights_bf = (raised / denominator).astype(jnp.bfloat16)
        block_out = jnp.einsum('kgqs,skd->qkgd', weights_bf.astype(jnp.float32), value_block.astype(jnp.float32))
        return block_out.reshape(block_rows, ATT_HEADS * HD).astype(jnp.bfloat16)
    blocks = lax.map(one_block, jnp.arange(seq_len // block_rows, dtype=jnp.int32))
    return blocks.reshape(seq_len, ATT_HEADS * HD)

def advance(state_now, item_pair):
    factor_now, term_now = item_pair
    return (factor_now[:, None, None] * state_now + term_now, state_now)

def retain_all(query_rot, key_rot, value_f, decay_log, init_state):
    seq_len = query_rot.shape[0]
    block_count = seq_len // RET_BLOCK

    def heads_first(values, width):
        return jnp.transpose(values.reshape(block_count, RET_BLOCK, RET_HEADS, width), (2, 0, 1, 3))
    query_h = heads_first(query_rot, RK)
    key_h = heads_first(key_rot, RK)
    value_h = heads_first(value_f, RV)
    block_logs = decay_log.reshape(RET_HEADS, block_count, RET_BLOCK)
    cumul = jnp.cumsum(block_logs, axis=-1)
    block_log = cumul[..., -1]
    inner_w = jnp.einsum('hbnk,hbmk->hbnm', query_h, key_h, precision=HIGHEST) * jnp.exp(-jnp.abs(cumul[..., :, None] - cumul[..., None, :]))
    local_out = jnp.einsum('hbnm,hbmv->hbnv', inner_w, value_h, precision=HIGHEST)
    fwd_terms = jnp.einsum('hbmk,hbmv->bhkv', key_h * jnp.exp(block_log[..., None] - cumul)[..., None], value_h, precision=HIGHEST)
    bwd_terms = jnp.einsum('hbmk,hbmv->bhkv', key_h * jnp.exp(cumul)[..., None], value_h, precision=HIGHEST)
    factors = jnp.exp(block_log).T
    _, fwd_in = lax.scan(advance, init_state[0], (factors, fwd_terms))
    _, bwd_in = lax.scan(advance, init_state[1], (factors, bwd_terms), reverse=True)
    cross_out = jnp.exp(cumul)[..., None] * jnp.einsum('hbnk,bhkv->hbnv', query_h, fwd_in, precision=HIGHEST)
    cross_out = cross_out + jnp.exp(block_log[..., None] - cumul)[..., None] * jnp.einsum('hbnk,bhkv->hbnv', query_h, bwd_in, precision=HIGHEST)
    combined = local_out + cross_out
    centered = combined - lax.optimization_barrier(jnp.mean(combined, axis=-1, keepdims=True))
    normed = centered * lax.rsqrt(lax.optimization_barrier(jnp.mean(centered * centered, axis=-1, keepdims=True)) + NORM_EPS)
    return jnp.transpose(normed, (1, 2, 0, 3)).reshape(seq_len, RET_HEADS * RV)

def reference(tokens, norm_gain, att_query, att_key, att_value, ret_query, ret_key, ret_value, ret_gate, att_sink, decay_log, init_state, out_att, out_ret):
    seq_len = tokens.shape[0]
    tokens_f = tokens.astype(jnp.float32)
    inv_rms = lax.rsqrt(lax.optimization_barrier(jnp.mean(tokens_f * tokens_f, axis=-1, keepdims=True)) + NORM_EPS)
    normed = (tokens_f * norm_gain.astype(jnp.float32)[None, :]).astype(jnp.bfloat16)

    def project(weight):
        return (jnp.dot(normed, weight, preferred_element_type=jnp.float32) * inv_rms).astype(jnp.bfloat16)
    attended = attend_all(project(att_query), project(att_key), project(att_value), att_sink)
    positions = jnp.arange(seq_len, dtype=jnp.int32)
    query_rot = rotated(project(ret_query).astype(jnp.float32).reshape(seq_len, RET_HEADS, RK), positions)
    key_rot = rotated(project(ret_key).astype(jnp.float32).reshape(seq_len, RET_HEADS, RK), positions) * RK ** (-0.5)
    value_f = project(ret_value).astype(jnp.float32).reshape(seq_len, RET_HEADS, RV)
    retained = retain_all(query_rot, key_rot, value_f, decay_log, init_state)
    gate_f = project(ret_gate).astype(jnp.float32)
    ret_out = (jax.nn.silu(gate_f) * retained).astype(jnp.bfloat16)
    att_width = ATT_HEADS * HD // N_TP
    ret_width = RET_HEADS * RV // N_TP
    summed = jnp.zeros((seq_len, D), jnp.float32)
    for group_index in range(N_TP):
        att_lo = group_index * att_width
        ret_lo = group_index * ret_width
        partial_sum = jnp.dot(attended[:, att_lo:att_lo + att_width], out_att[att_lo:att_lo + att_width], preferred_element_type=jnp.float32)
        partial_sum = partial_sum + jnp.dot(ret_out[:, ret_lo:ret_lo + ret_width], out_ret[ret_lo:ret_lo + ret_width], preferred_element_type=jnp.float32)
        rounded = lax.optimization_barrier(partial_sum.astype(jnp.bfloat16))
        summed = summed + rounded.astype(jnp.float32)
    return summed.astype(jnp.bfloat16)
```

```python
import functools

import jax
import jax.numpy as jnp
import numpy as np
from jax import lax
from jax.experimental import pallas as pl
from jax.experimental.pallas import tpu as pltpu
from jax.sharding import PartitionSpec as P

HD = 64
RK = 64
RV = 128
WINDOW = 128
NORM_EPS = 1e-06
ROPE_BASE = 10000.0
NEG = -1e30
EXTRA = 16
CHUNKS = 4
F32 = jnp.float32
BF16 = jnp.bfloat16

VMEM = pl.BlockSpec(memory_space=pltpu.VMEM)
SMEM = pl.BlockSpec(memory_space=pltpu.SMEM)
ANY = pl.BlockSpec(memory_space=pl.ANY)


def cost(flops, nbytes):
    return pl.CostEstimate(flops=int(flops), bytes_accessed=int(nbytes), transcendentals=0)


def dot(a, b):
    return jnp.dot(a, b, preferred_element_type=F32)


def dot_t(a, b):
    return lax.dot_general(a, b, (((1,), (1,)), ((), ())), preferred_element_type=F32)


def t_dot(a, b):
    return lax.dot_general(a, b, (((0,), (0,)), ((), ())), preferred_element_type=F32)


def project_kernel(n_blocks, n_w, parts, *refs):
    idx_ref, gain_ref = refs[:2]
    blocks = refs[2 : 2 + n_blocks]
    cos_ref, sin_ref, perm_ref = refs[2 + n_blocks : 5 + n_blocks]
    w_refs = refs[5 + n_blocks : 5 + n_blocks + n_w]
    out_ref = refs[5 + n_blocks + n_w]
    xn, wbuf, sems = refs[-3:]
    width = blocks[0].shape[1]
    copies = []
    for w_ref, (group, low) in zip(w_refs, parts):
        dst = wbuf.at[group]
        if w_ref.shape[1] != wbuf.shape[2]:
            dst = wbuf.at[group, :, pl.ds(low, w_ref.shape[1])]
        copy = pltpu.make_async_copy(w_ref, dst, sems.at[group])
        copy.start()
        copies.append(copy)
    rows = xn.shape[0]
    squares = jnp.zeros((rows, 1), F32)
    for i, block in enumerate(blocks):
        start = pl.multiple_of(idx_ref[i] * width, width)
        values = block[...].astype(F32)
        squares = squares + jnp.sum(values * values, axis=1, keepdims=True)
        xn[:, pl.ds(start, width)] = (values * gain_ref[:, pl.ds(start, width)]).astype(BF16)
    inv = lax.rsqrt(squares / (width * n_blocks) + NORM_EPS)

    def group_step(group, carry):
        pltpu.make_async_copy(wbuf.at[group], wbuf.at[group], sems.at[group]).wait()
        scale = jnp.where(group == 0, HD ** (-0.5), 1.0).astype(F32)
        out_ref[group] = (dot(xn[...], wbuf[group]) * inv).astype(BF16) * scale.astype(BF16)
        return carry

    lax.fori_loop(0, out_ref.shape[0], group_step, 0)
    raw = out_ref[2]
    turned = raw.astype(F32) * cos_ref[...] + dot(raw, perm_ref[...]) * sin_ref[...]
    out_ref[2] = turned.astype(BF16)


def project(idx, gain, blocks, cos, sin, perm, weights, parts, chunk, rows, interpret_width):
    group_width = interpret_width
    depth = gain.shape[1]
    in_specs = [SMEM, VMEM]
    for block in blocks:
        pick = chunk if block.shape[0] != rows else 0
        in_specs.append(pl.BlockSpec((rows, block.shape[1]), lambda i, pick=pick: (pick, 0)))
    for _ in range(2):
        in_specs.append(pl.BlockSpec((rows, group_width), lambda i: (chunk, 0)))
    in_specs.append(VMEM)
    in_specs += [ANY] * len(weights)
    return pl.pallas_call(
        functools.partial(project_kernel, len(blocks), len(weights), parts),
        grid=(1,),
        out_shape=jax.ShapeDtypeStruct((5, rows, group_width), BF16),
        in_specs=in_specs,
        out_specs=pl.BlockSpec((5, rows, group_width), lambda i: (0, 0, 0)),
        scratch_shapes=[
            pltpu.VMEM((rows, depth), BF16),
            pltpu.VMEM((5, depth, group_width), BF16),
            pltpu.SemaphoreType.DMA((5,)),
        ],
        cost_estimate=cost(2 * rows * depth * 5 * group_width // 4, 7 << 20),
        name="project",
    )(idx, gain, *blocks, cos, sin, perm, *weights)


def attend_kernel(n_chunks, kv_local, groups, seq_len, *refs):
    offset_ref, sink_ref = refs[:2]
    q_refs = refs[2 : 2 + n_chunks]
    kv_refs = refs[2 + n_chunks : 2 + 2 * n_chunks]
    low_ref, high_ref, out_ref = refs[2 + 2 * n_chunks : 5 + 2 * n_chunks]
    qbuf, kvbuf = refs[-2:]
    rows = q_refs[0].shape[1]
    total = rows * n_chunks
    kv_cols = kv_local * HD
    kvbuf[0:WINDOW] = low_ref[...]
    for c in range(n_chunks):
        kvbuf[pl.ds(WINDOW + c * rows, rows)] = kv_refs[c][0]
        qbuf[pl.ds(c * rows, rows)] = q_refs[c][0]
    kvbuf[pl.ds(WINDOW + total, WINDOW)] = high_ref[...]
    block = WINDOW
    span = block + 2 * WINDOW
    row = lax.broadcasted_iota(jnp.int32, (block, span), 0)
    col = lax.broadcasted_iota(jnp.int32, (block, span), 1)
    band = (col >= row) & (col <= row + 2 * WINDOW)

    def step(i, carry):
        first = pl.multiple_of(i * block, block)
        q = qbuf[pl.ds(first, block)]
        kv = kvbuf[pl.ds(first, span)]
        pos = col + (offset_ref[0] + first - WINDOW)
        allowed = band & (pos >= 0) & (pos < seq_len)
        outs = []
        for g in range(kv_local):
            k = kv[:, g * HD : (g + 1) * HD]
            v = kv[:, kv_cols + g * HD : kv_cols + (g + 1) * HD]
            vo = jnp.concatenate([v, jnp.ones((span, 128 - HD), BF16)], axis=1)
            for j in range(groups):
                h = g * groups + j
                s = jnp.where(allowed, dot_t(q[:, h * HD : (h + 1) * HD], k), NEG)
                sink = sink_ref[h]
                top = jnp.maximum(jnp.max(s, axis=1, keepdims=True), sink)
                p = jnp.exp(s - top).astype(BF16)
                o = dot(p, vo)
                den = o[:, HD : HD + 1] + jnp.exp(sink - top)
                outs.append(o[:, :HD] / den)
        out_ref[pl.ds(first, block)] = jnp.concatenate(outs, axis=1).astype(BF16)
        return carry

    lax.fori_loop(0, total // block, step, 0)


def group_spec(group, rows, width):
    return pl.BlockSpec((1, rows, width), lambda i: (group, 0, 0))


def attend(offset, sink, proj, low, high, kv_local, groups, seq_len):
    n = len(proj)
    _, rows, width = proj[0].shape
    total = rows * n
    return pl.pallas_call(
        functools.partial(attend_kernel, n, kv_local, groups, seq_len),
        grid=(1,),
        out_shape=jax.ShapeDtypeStruct((total, width), BF16),
        in_specs=[SMEM, SMEM]
        + [group_spec(0, rows, width)] * n
        + [group_spec(1, rows, width)] * n
        + [VMEM, VMEM],
        out_specs=pl.BlockSpec((total, width), lambda i: (0, 0)),
        scratch_shapes=[
            pltpu.VMEM((total, width), BF16),
            pltpu.VMEM((total + 2 * WINDOW, width), BF16),
        ],
        cost_estimate=cost(1.5e9, 3 << 20),
        name="attend",
    )(offset, sink, *proj, *proj, low, high)


def totals_kernel(n_chunks, ret_local, n_sp, *refs):
    me_ref, ccol_ref, end_ref = refs[:3]
    r_refs = refs[3 : 3 + n_chunks]
    v_refs = refs[3 + n_chunks : 3 + 2 * n_chunks]
    out_ref = refs[-1]
    rows = r_refs[0].shape[1]
    sums = [jnp.zeros((RK, 2 * RV), F32) for _ in range(ret_local)]
    for c in range(n_chunks):
        k_all = r_refs[c][0]
        v_all = v_refs[c][0]
        for h in range(ret_local):
            col = ccol_ref[pl.ds(c * rows, rows), h : h + 1]
            v = v_all[:, h * RV : (h + 1) * RV].astype(F32)
            both = jnp.concatenate(
                [v * jnp.exp(end_ref[h] - col), v * jnp.exp(col)], axis=1
            ).astype(BF16)
            k = k_all[:, (ret_local + h) * RK : (ret_local + h + 1) * RK]
            sums[h] = sums[h] + t_dot(k, both)
    me = me_ref[0]
    line = lax.broadcasted_iota(jnp.int32, (EXTRA, RV), 0)
    for h in range(ret_local):
        end = jnp.full((EXTRA, RV), end_ref[h], F32)
        d0 = end.astype(BF16).astype(F32)
        d1 = (end - d0).astype(BF16).astype(F32)
        d2 = end - d0 - d1
        extra = jnp.where(line == 0, d0, jnp.where(line == 1, d1, jnp.where(line == 2, d2, 0.0)))
        fwd = jnp.concatenate([sums[h][:, :RV], extra], axis=0).astype(BF16)
        bwd = jnp.concatenate([sums[h][:, RV:], extra], axis=0).astype(BF16)
        for j in range(n_sp):
            out_ref[j, h] = jnp.where(j > me, fwd, bwd)


def totals(me, ccol, end, proj, ret_local, n_sp):
    n = len(proj)
    _, rows, width = proj[0].shape
    return pl.pallas_call(
        functools.partial(totals_kernel, n, ret_local, n_sp),
        grid=(1,),
        out_shape=jax.ShapeDtypeStruct((n_sp, ret_local, RK + EXTRA, RV), BF16),
        in_specs=[SMEM, VMEM, SMEM]
        + [group_spec(2, rows, width)] * n
        + [group_spec(3, rows, width)] * n,
        out_specs=pl.BlockSpec((n_sp, ret_local, RK + EXTRA, RV), lambda i: (0, 0, 0, 0)),
        cost_estimate=cost(0.3e9, 2 << 20),
        name="totals",
    )(me, ccol, end, *proj, *proj)


def local_kernel(n_chunks, ret_local, *refs):
    ccol_ref, crow_ref = refs[:2]
    r_refs = refs[2 : 2 + n_chunks]
    v_refs = refs[2 + n_chunks : 2 + 2 * n_chunks]
    out_ref = refs[2 + 2 * n_chunks]
    rbuf, vbuf = refs[-2:]
    rows = r_refs[0].shape[1]
    total = rows * n_chunks
    for c in range(n_chunks):
        rbuf[pl.ds(c * rows, rows)] = r_refs[c][0]
        vbuf[pl.ds(c * rows, rows)] = v_refs[c][0]
    block = min(128, rows)

    def step(i, carry):
        first = pl.multiple_of(i * block, block)
        for h in range(ret_local):
            q = rbuf[pl.ds(first, block), h * RK : (h + 1) * RK]
            k = rbuf[:, (ret_local + h) * RK : (ret_local + h + 1) * RK]
            gap = ccol_ref[pl.ds(first, block), h : h + 1] - crow_ref[h : h + 1, :]
            w = (dot_t(q, k) * jnp.exp(-jnp.abs(gap))).astype(BF16)
            out_ref[pl.ds(first, block), h * RV : (h + 1) * RV] = dot(
                w, vbuf[:, h * RV : (h + 1) * RV]
            )
        return carry

    lax.fori_loop(0, total // block, step, 0)


def local(ccol, crow, proj, ret_local):
    n = len(proj)
    _, rows, width = proj[0].shape
    total = rows * n
    return pl.pallas_call(
        functools.partial(local_kernel, n, ret_local),
        grid=(1,),
        out_shape=jax.ShapeDtypeStruct((total, width), F32),
        in_specs=[VMEM, VMEM]
        + [group_spec(2, rows, width)] * n
        + [group_spec(3, rows, width)] * n,
        out_specs=pl.BlockSpec((total, width), lambda i: (0, 0)),
        scratch_shapes=[pltpu.VMEM((total, width), BF16), pltpu.VMEM((total, width), BF16)],
        cost_estimate=cost(1e9, 3 << 20),
        name="local",
    )(ccol, crow, *proj, *proj)


def cross_kernel(n_chunks, ret_local, n_sp, *refs):
    me_ref, end_ref, ccol_ref, got_ref, init_ref, loc_ref = refs[:6]
    r_refs = refs[6 : 6 + n_chunks]
    g_refs = refs[6 + n_chunks : 6 + 2 * n_chunks]
    out_ref = refs[-1]
    rows = r_refs[0].shape[1]
    me = me_ref[0]
    for h in range(ret_local):
        ends = []
        for j in range(n_sp):
            tail = got_ref[j, h, RK : RK + EXTRA, :].astype(F32)
            ends.append(jnp.sum(tail, axis=0, keepdims=True))
        fwd = jnp.zeros((RK, RV), F32)
        run = jnp.zeros((1, RV), F32)
        for j in range(n_sp - 1, -1, -1):
            here = j < me
            term = jnp.exp(run) * got_ref[j, h, 0:RK, :].astype(F32)
            fwd = fwd + jnp.where(here, term, 0.0)
            run = run + jnp.where(here, ends[j], 0.0)
        fwd = fwd + jnp.exp(run) * init_ref[0, h]
        bwd = jnp.zeros((RK, RV), F32)
        run = jnp.zeros((1, RV), F32)
        for j in range(n_sp):
            here = j > me
            term = jnp.exp(run) * got_ref[j, h, 0:RK, :].astype(F32)
            bwd = bwd + jnp.where(here, term, 0.0)
            run = run + jnp.where(here, ends[j], 0.0)
        bwd = bwd + jnp.exp(run) * init_ref[1, h]
        state = jnp.concatenate([fwd, bwd], axis=1).astype(BF16)
        for c in range(n_chunks):
            here = pl.ds(c * rows, rows)
            q = r_refs[c][0, :, h * RK : (h + 1) * RK]
            both = dot(q, state)
            col = ccol_ref[here, h : h + 1]
            ret = (
                loc_ref[here, h * RV : (h + 1) * RV]
                + jnp.exp(col) * both[:, :RV]
                + jnp.exp(end_ref[h] - col) * both[:, RV:]
            )
            centered = ret - jnp.mean(ret, axis=1, keepdims=True)
            scale = lax.rsqrt(jnp.mean(centered * centered, axis=1, keepdims=True) + NORM_EPS)
            gate = g_refs[c][0, :, h * RV : (h + 1) * RV].astype(F32)
            gated = gate / (1.0 + jnp.exp(-gate))
            out_ref[here, h * RV : (h + 1) * RV] = (gated * (centered * scale)).astype(BF16)


def cross(me, end, ccol, got, init, loc, proj, ret_local, n_sp):
    n = len(proj)
    _, rows, width = proj[0].shape
    total = rows * n
    return pl.pallas_call(
        functools.partial(cross_kernel, n, ret_local, n_sp),
        grid=(1,),
        out_shape=jax.ShapeDtypeStruct((total, width), BF16),
        in_specs=[SMEM, SMEM, VMEM, VMEM, VMEM, VMEM]
        + [group_spec(2, rows, width)] * n
        + [group_spec(4, rows, width)] * n,
        out_specs=pl.BlockSpec((total, width), lambda i: (0, 0)),
        cost_estimate=cost(0.5e9, 4 << 20),
        name="cross",
    )(me, end, ccol, got, init, loc, *proj, *proj)


def output_kernel(n_src, *refs):
    att = refs[:n_src]
    ret = refs[n_src : 2 * n_src]
    weights = refs[2 * n_src : 3 * n_src]
    out_ref = refs[3 * n_src]
    width = att[0].shape[1]
    total = jnp.zeros(out_ref.shape, F32)
    for a, r, w in zip(att, ret, weights):
        total = total + dot(a[...], w[0:width]) + dot(r[...], w[width : 2 * width])
    out_ref[...] = total.astype(BF16)


def output(att, ret, weights):
    n_src = len(att)
    total, width = att[0].shape
    cols = weights[0].shape[1]
    rows = min(256, total)
    data = pl.BlockSpec((rows, width), lambda i: (i, 0))
    return pl.pallas_call(
        functools.partial(output_kernel, n_src),
        grid=(total // rows,),
        out_shape=jax.ShapeDtypeStruct((total, cols), BF16),
        in_specs=[data] * (2 * n_src) + [VMEM] * n_src,
        out_specs=pl.BlockSpec((rows, cols), lambda i: (i, 0)),
        cost_estimate=cost(1e9, 8 << 20),
        name="output",
    )(*att, *ret, *weights)


def core_swap(value):
    n = lax.axis_size("tp")
    return lax.ppermute(value, "tp", [(i, i ^ 1) for i in range(n)])


def chip_turn(value, by):
    n = lax.axis_size("tp")
    return lax.ppermute(value, "tp", [(i, (i + 2 * by) % n) for i in range(n)])


def gather_tp(value):
    blocks = [value, core_swap(value)]
    for by in range(1, lax.axis_size("tp") // 2):
        far = chip_turn(value, by)
        blocks += [far, core_swap(far)]
    return blocks


def sources():
    n = lax.axis_size("tp")
    me = lax.axis_index("tp")
    out = [me, me ^ 1]
    for by in range(1, n // 2):
        far = (me + n - 2 * by) % n
        out += [far, far ^ 1]
    return out


def output_weights(out_att, out_ret):
    n_tp, n_sp = lax.axis_size("tp"), lax.axis_size("sp")
    tp, sp = lax.axis_index("tp"), lax.axis_index("sp")
    stacked = jnp.concatenate([out_att, out_ret], axis=0)
    depth, model = stacked.shape
    cols = model // n_tp
    own = lax.dynamic_slice_in_dim(stacked, tp * cols, cols, axis=1)
    peer = core_swap(lax.dynamic_slice_in_dim(stacked, (tp ^ 1) * cols, cols, axis=1))
    share = depth // n_sp
    slab = lax.dynamic_slice_in_dim(stacked, sp * share, share, axis=0)
    slab = jnp.transpose(slab.reshape(share, n_tp, cols), (1, 0, 2))
    slab = lax.all_to_all(slab, "tp", 0, 0, tiled=True)
    far = sources()[2:]
    mine = jnp.concatenate([lax.dynamic_slice_in_dim(slab, s, 1, axis=0) for s in far], axis=0)
    spread = jnp.broadcast_to(mine[None], (n_sp,) + mine.shape)
    spread = lax.all_to_all(spread, "sp", 0, 0, tiled=True)
    spread = jnp.transpose(spread, (1, 0, 2, 3)).reshape(len(far), depth, cols)
    return [own, peer] + [spread[i] for i in range(len(far))]


def body(
    tokens,
    norm_gain,
    att_query,
    att_key,
    att_value,
    ret_query,
    ret_key,
    ret_value,
    ret_gate,
    att_sink,
    decay_log,
    init_state,
    out_att,
    out_ret,
):
    n_sp = lax.axis_size("sp")
    me = lax.axis_index("sp")
    total = tokens.shape[0]
    seq_len = total * n_sp
    width = att_query.shape[1]
    half = width // 2
    kv_local = att_key.shape[1] // HD
    groups = att_sink.shape[0] // kv_local
    ret_local = decay_log.shape[0]
    rows = total // CHUNKS

    pieces = [tokens[c * rows : (c + 1) * rows] for c in range(CHUNKS)]
    order = [0, CHUNKS - 1] + list(range(1, CHUNKS - 1))
    near = core_swap(tokens)
    far = {c: [] for c in order}
    for c in order:
        for by in range(1, lax.axis_size("tp") // 2):
            block = chip_turn(pieces[c], by)
            far[c] += [block, core_swap(block)]
    idx = jnp.stack(sources()).astype(jnp.int32)

    position = (me * total + jnp.arange(total, dtype=jnp.int32)).astype(F32)
    inverse = ROPE_BASE ** (-2.0 * jnp.arange(RK // 2, dtype=F32) / RK)
    angles = position[:, None] * inverse[None, :]
    cos, sin = lax.optimization_barrier((jnp.cos(angles), jnp.sin(angles)))
    key_scale = RK ** (-0.5)
    cos = jnp.concatenate([cos] * (2 * ret_local) + [cos * key_scale] * (2 * ret_local), axis=1)
    sin = jnp.concatenate(
        [-sin, sin] * ret_local + [-sin * key_scale, sin * key_scale] * ret_local, axis=1
    )
    lane = np.arange(width)
    perm = np.zeros((width, width), np.float32)
    perm[lane ^ (RK // 2), lane] = 1.0
    perm = jnp.asarray(perm, BF16)

    if half % 128 == 0:
        weights = [att_query, att_key, att_value, ret_query, ret_key, ret_value, ret_gate]
        parts = [(0, 0), (1, 0), (1, half), (2, 0), (2, half), (3, 0), (4, 0)]
    else:
        weights = [
            att_query,
            jnp.concatenate([att_key, att_value], axis=1),
            jnp.concatenate([ret_query, ret_key], axis=1),
            ret_value,
            ret_gate,
        ]
        parts = [(i, 0) for i in range(5)]
    gain = norm_gain[None, :]
    proj = [None] * CHUNKS
    for c in order:
        blocks = [tokens, near] + far[c]
        proj[c] = project(idx, gain, blocks, cos, sin, perm, weights, parts, c, rows, width)

    forward = [(i, (i + 1) % n_sp) for i in range(n_sp)]
    backward = [(target, source) for source, target in forward]
    low = lax.ppermute(proj[-1][1, rows - WINDOW :], "sp", forward)
    high = lax.ppermute(proj[0][1, :WINDOW], "sp", backward)

    crow = jnp.cumsum(decay_log, axis=1)
    ccol = crow.T
    end = crow[:, -1]
    me_arr = me.reshape(1).astype(jnp.int32)
    offset = (me * total).reshape(1).astype(jnp.int32)

    sent = totals(me_arr, ccol, end, proj, ret_local, n_sp)
    got = lax.all_to_all(sent, "sp", 0, 0, tiled=True)
    attended = attend(offset, att_sink, proj, low, high, kv_local, groups, seq_len)
    att_blocks = gather_tp(attended)
    loc = local(ccol, crow, proj, ret_local)
    kept = cross(me_arr, end, ccol, got, init_state, loc, proj, ret_local, n_sp)
    ret_blocks = gather_tp(kept)
    out_w = output_weights(out_att, out_ret)
    return output(att_blocks, ret_blocks, out_w)


def solution(mesh):
    in_specs = (
        P("sp", "tp"),
        P(),
        P(None, "tp"),
        P(None, "tp"),
        P(None, "tp"),
        P(None, "tp"),
        P(None, "tp"),
        P(None, "tp"),
        P(None, "tp"),
        P("tp"),
        P("tp", "sp"),
        P(None, "tp", None, None),
        P("tp", None),
        P("tp", None),
    )
    out_specs = P("sp", "tp")
    return jax.shard_map(body, mesh=mesh, in_specs=in_specs, out_specs=out_specs, check_vma=False)
```

```python
import functools
import math

import jax
import jax.numpy as jnp
import numpy as np
from jax import lax
from jax.experimental import pallas as pl
from jax.experimental.pallas import tpu as pltpu
from jax.sharding import PartitionSpec as P


HD = 64
RK = 64
RV = 128
WINDOW = 128
NORM_EPS = 1e-06
ROPE_BASE = 10000.0
NEG = -1e30
EXTRA = 16
CHUNKS = ((0, 1), (1, 1), (2, 2))
ORDER = (2, 0, 1)
TABLE = 32
F32 = jnp.float32
BF16 = jnp.bfloat16

VMEM = pl.BlockSpec(memory_space=pltpu.VMEM)
SMEM = pl.BlockSpec(memory_space=pltpu.SMEM)
ANY = pl.BlockSpec(memory_space=pl.ANY)
PARAMS = pltpu.CompilerParams(vmem_limit_bytes=16 << 20)


def cost(flops, nbytes):
    return pl.CostEstimate(flops=int(flops), bytes_accessed=int(nbytes), transcendentals=0)


def dot(a, b):
    return jnp.dot(a, b, preferred_element_type=F32)


def dot_t(a, b):
    return lax.dot_general(a, b, (((1,), (1,)), ((), ())), preferred_element_type=F32)


def t_dot(a, b):
    return lax.dot_general(a, b, (((0,), (0,)), ((), ())), preferred_element_type=F32)


def split_kernel(n_pieces, n_far, *refs):
    tokens, att, ret = refs[:3]
    pieces = refs[3 : 3 + n_pieces]
    slabs = refs[3 + n_pieces : 3 + n_pieces + n_far]
    sems = refs[-1]
    n_tp = lax.axis_size("tp")
    tp, sp = lax.axis_index("tp"), lax.axis_index("sp")
    chips = n_tp // 2
    copies = []
    for by in range(1, chips):
        slab = slabs[by - 1]
        share, width = slab.shape[0] // 2, slab.shape[1]
        target = lax.rem(tp // 2 + by, chips)
        rows = pl.ds(pl.multiple_of(sp * share, share), share)
        cols = pl.ds(pl.multiple_of(target * width, width), width)
        for i, ref in enumerate((att, ret)):
            dst = slab.at[pl.ds(i * share, share)]
            copies.append(pltpu.make_async_copy(ref.at[rows, cols], dst, sems.at[2 * by - 2 + i]))
    for copy in copies:
        copy.start()
    for c, piece in enumerate(pieces):
        first = CHUNKS[c][0] * tokens.shape[0] // 4
        piece[...] = tokens[first : first + piece.shape[0]]
    for copy in copies:
        copy.wait()


def split(tokens, att, ret):
    total, cols = tokens.shape
    chips = lax.axis_size("tp") // 2
    share = att.shape[0] // lax.axis_size("sp")
    shapes = [jax.ShapeDtypeStruct((n * total // 4, cols), BF16) for _, n in CHUNKS]
    shapes += [jax.ShapeDtypeStruct((2 * share, 2 * cols), BF16)] * (chips - 1)
    if share % 16:
        rows = lax.axis_index("sp") * share
        out = [tokens[f * total // 4 : (f + n) * total // 4] for f, n in CHUNKS]
        for by in range(1, chips):
            target = lax.rem(lax.axis_index("tp") // 2 + by, chips) * 2 * cols
            parts = [lax.dynamic_slice(w, (rows, target), (share, 2 * cols)) for w in (att, ret)]
            out.append(jnp.concatenate(parts, axis=0))
    else:
        out = pl.pallas_call(
            functools.partial(split_kernel, len(CHUNKS), chips - 1),
            out_shape=tuple(shapes),
            in_specs=[VMEM, ANY, ANY],
            out_specs=(VMEM,) * len(shapes),
            scratch_shapes=[pltpu.SemaphoreType.DMA((2 * chips,))],
            cost_estimate=cost(0.1e9, 3 << 20),
            compiler_params=PARAMS,
            name="split",
        )(tokens, att, ret)
    return out[: len(CHUNKS)], out[len(CHUNKS) :]


def repeat_kernel(*refs):
    out_ref = refs[-1]
    for s in range(out_ref.shape[0]):
        for i, ref in enumerate(refs[:-1]):
            out_ref[s, i] = ref[...]


def repeat(slabs, count):
    return pl.pallas_call(
        repeat_kernel,
        out_shape=jax.ShapeDtypeStruct((count, len(slabs)) + slabs[0].shape, BF16),
        in_specs=[VMEM] * len(slabs),
        out_specs=VMEM,
        cost_estimate=cost(0.1e9, 1 << 20),
        compiler_params=PARAMS,
        name="repeat",
    )(*slabs)


def prepare_kernel(log_ref, row_ref, col_ref, cos_ref, sin_ref):
    total = log_ref.shape[1]
    heads = log_ref.shape[0]
    sums = jnp.concatenate([log_ref[...], jnp.zeros((8 - heads, total), F32)], axis=0)
    lane = lax.broadcasted_iota(jnp.int32, sums.shape, 1)
    step = 1
    while step < total:
        sums = sums + jnp.where(lane >= step, pltpu.roll(sums, step, 1), 0.0)
        step *= 2
    row_ref[...] = sums
    col_ref[...] = sums.T
    rows, lanes = cos_ref.shape
    row = lax.broadcasted_iota(jnp.int32, (rows, lanes), 0)
    pair = lax.broadcasted_iota(jnp.int32, (rows, lanes), 1) & (RK // 2 - 1)
    count = total // TABLE
    place = jnp.where(row < count, lax.axis_index("sp") * total + TABLE * row, row - count)
    inverse = jnp.exp(pair.astype(F32) * (-2.0 * math.log(ROPE_BASE) / RK))
    angles = place.astype(F32) * inverse
    cos_ref[...] = jnp.cos(angles)
    sin_ref[...] = jnp.sin(angles)


def prepare(log):
    heads, total = log.shape
    table = jax.ShapeDtypeStruct((total // TABLE + TABLE, heads * RK), F32)
    return pl.pallas_call(
        prepare_kernel,
        out_shape=(
            jax.ShapeDtypeStruct((8, total), F32),
            jax.ShapeDtypeStruct((total, 8), F32),
            table,
            table,
        ),
        in_specs=[VMEM],
        out_specs=(VMEM,) * 4,
        cost_estimate=cost(0.1e9, 1 << 16),
        compiler_params=PARAMS,
        name="prepare",
    )(log)


def project_kernel(n_blocks, n_w, parts, first, ret_local, *refs):
    gain_ref, crow_ref, ccol_ref, swap_ref, mix_ref, cos_ref, sin_ref = refs[:7]
    blocks = refs[7 : 7 + n_blocks]
    w_refs = refs[7 + n_blocks : 7 + n_blocks + n_w]
    out_ref, sum_ref, low_ref, high_ref = refs[7 + n_blocks + n_w : 11 + n_blocks + n_w]
    xn, inv = refs[-2:]
    width = blocks[0].shape[1]
    rows = xn.shape[0]
    group_width = inv.shape[1]
    half = group_width // 2
    total = crow_ref.shape[1]
    mine = pl.ds(first, rows)
    starts = [pl.multiple_of(i * width, width) for i in sources()]
    tile = min(128, rows)
    lanes = min(128, width)
    for r in range(rows // tile):
        here = pl.ds(r * tile, tile)
        squares = jnp.zeros((tile, lanes), F32)
        for start, block in zip(starts, blocks):
            at = here if block.shape[0] == rows else pl.ds(first + r * tile, tile)
            for low in range(0, width, lanes):
                part = block[at, low : low + lanes].astype(F32)
                squares = squares + part * part
                col = pl.ds(pl.multiple_of(start + low, lanes), lanes)
                xn[here, col] = (part * gain_ref[:, col]).astype(BF16)
        mean = jnp.sum(squares, axis=1, keepdims=True) / (width * n_blocks)
        inv[here, :] = jnp.broadcast_to(lax.rsqrt(mean + NORM_EPS), (tile, group_width))
    count = total // TABLE
    cos_b, sin_b = cos_ref[count:], sin_ref[count:]
    cosines, sines = [], []
    for k in range(first // TABLE, (first + rows) // TABLE):
        cos_k, sin_k = cos_ref[k : k + 1], sin_ref[k : k + 1]
        cosines.append(cos_k * cos_b - sin_k * sin_b)
        sines.append(sin_k * cos_b + cos_k * sin_b)
    cosine = jnp.concatenate(cosines, axis=0)
    sine = jnp.concatenate(sines, axis=0)
    for group in (2, 3, 0, 1, 4):
        ws = [w[...] for w, (g, _) in zip(w_refs, parts) if g == group]
        w = ws[0] if len(ws) == 1 else jnp.concatenate(ws, axis=1)
        raw = (dot(xn[...], w) * inv[...]).astype(BF16)
        if group == 0:
            raw = (dot(raw, mix_ref[...]) * HD ** (-0.5)).astype(BF16)
        if group == 2:
            sides = []
            for low, scale in ((0, 1.0), (half, RK ** (-0.5))):
                side = raw[:, low : low + half]
                turned = side.astype(F32) * cosine + dot(side, swap_ref[...]) * sine
                sides.append((turned * scale).astype(BF16))
            keys = sides[1]
            raw = jnp.concatenate(sides, axis=1)
        if group == 3:
            for h in range(ret_local):
                col = ccol_ref[mine, h : h + 1]
                end = crow_ref[h : h + 1, total - 1 : total]
                v = raw[:, h * RV : (h + 1) * RV].astype(F32)
                both = jnp.concatenate([v * jnp.exp(end - col), v * jnp.exp(col)], axis=1)
                sum_ref[h] = t_dot(keys, both.astype(BF16))[h * RK : (h + 1) * RK]
        if group == 1:
            low_ref[...] = raw[rows - WINDOW :]
            high_ref[...] = raw[:WINDOW]
        out_ref[group] = raw


def project(gain, crow, ccol, swap, mix, cos, sin, blocks, weights, parts, first, rows, ret_local):
    width = mix.shape[0]
    depth = gain.shape[1]
    n = len(blocks)
    return pl.pallas_call(
        functools.partial(project_kernel, n, len(weights), parts, first, ret_local),
        out_shape=(
            jax.ShapeDtypeStruct((5, rows, width), BF16),
            jax.ShapeDtypeStruct((ret_local, RK, 2 * RV), F32),
            jax.ShapeDtypeStruct((WINDOW, width), BF16),
            jax.ShapeDtypeStruct((WINDOW, width), BF16),
        ),
        in_specs=[VMEM] * (n + 7 + len(weights)),
        out_specs=(VMEM,) * 4,
        scratch_shapes=[pltpu.VMEM((rows, depth), BF16), pltpu.VMEM((rows, width), F32)],
        cost_estimate=cost(2 * rows * depth * 5 * width // 4, 7 << 20),
        compiler_params=PARAMS,
        name="project",
    )(gain, crow, ccol, swap, mix, cos, sin, *blocks, *weights)


def attend_kernel(n_chunks, kv_local, groups, seq_len, *refs):
    sink_ref = refs[0]
    proj = refs[1 : 1 + n_chunks]
    low_ref, high_ref, out_ref = refs[1 + n_chunks : 4 + n_chunks]
    qbuf, kbuf, vbuf, mask = refs[-4:]
    total = sum(ref.shape[1] for ref in proj)
    offset = lax.axis_index("sp") * total
    kv_cols = kv_local * HD
    block = WINDOW
    span = block + 2 * WINDOW
    pieces = [(0, low_ref[...])]
    at = 0
    for ref in proj:
        pieces.append((WINDOW + at, ref[1]))
        qbuf[pl.ds(at, ref.shape[1])] = ref[0]
        at += ref.shape[1]
    pieces.append((WINDOW + total, high_ref[...]))
    for first, kv in pieces:
        here = pl.ds(first, kv.shape[0])
        kbuf[here] = kv[:, :kv_cols]
        vbuf[0:kv_cols, here] = kv[:, kv_cols:].T
    vbuf[kv_cols:] = jnp.ones((vbuf.shape[0] - kv_cols, vbuf.shape[1]), BF16)
    row = lax.broadcasted_iota(jnp.int32, (span, block), 1)
    col = lax.broadcasted_iota(jnp.int32, (span, block), 0)
    band = (col >= row) & (col <= row + 2 * WINDOW)
    for i, first in enumerate((0, block, total - block)):
        pos = col + (offset + first - WINDOW)
        allowed = band & (pos >= 0) & (pos < seq_len)
        one = jnp.where(allowed, 0.0, NEG)
        mask[i] = jnp.concatenate([one] * groups, axis=1)
    lane = lax.broadcasted_iota(jnp.int32, (block, kv_cols), 1)
    n_steps = total // block

    def step(i, carry):
        first = pl.multiple_of(i * block, block)
        q = qbuf[pl.ds(first, block)]
        k = kbuf[pl.ds(first, span)]
        kind = jnp.where(i == 0, 0, jnp.where(i == n_steps - 1, 2, 1))
        bias = mask[kind]
        scores = []
        for g in range(kv_local):
            mine = (lane >= g * HD) & (lane < (g + 1) * HD)
            tiles = []
            for j in range(groups):
                tile = q[:, j * kv_cols : (j + 1) * kv_cols]
                tiles.append(jnp.where(mine, tile, jnp.zeros_like(tile)))
            scores.append(dot_t(k, jnp.concatenate(tiles, axis=0)))
        weights = []
        rests = []
        for g in range(kv_local):
            s = scores[g] + bias
            sink = jnp.concatenate(
                [jnp.full((1, block), sink_ref[g * groups + j], F32) for j in range(groups)], axis=1
            )
            top = jnp.maximum(jnp.max(s, axis=0, keepdims=True), sink)
            weights.append(jnp.exp(s - top).astype(BF16))
            rests.append(jnp.exp(sink - top))
        outs = []
        for g in range(kv_local):
            v = vbuf[g * HD : (g + 1) * HD, pl.ds(first, span)]
            ones = vbuf[kv_cols : kv_cols + 16, pl.ds(first, span)]
            o = dot(jnp.concatenate([v, ones], axis=0), weights[g])
            o = o[:HD] / (o[HD : HD + 1] + rests[g])
            outs += [o[:, j * block : (j + 1) * block] for j in range(groups)]
        out_ref[pl.ds(first, block)] = jnp.concatenate(outs, axis=0).T.astype(BF16)
        return carry

    lax.fori_loop(0, n_steps, step, 0, unroll=n_steps)


def attend(sink, proj, low, high, kv_local, groups, seq_len):
    n = len(proj)
    width = proj[0].shape[2]
    total = sum(p.shape[1] for p in proj)
    kv_cols = kv_local * HD
    return pl.pallas_call(
        functools.partial(attend_kernel, n, kv_local, groups, seq_len),
        out_shape=jax.ShapeDtypeStruct((total, width), BF16),
        in_specs=[SMEM] + [VMEM] * (n + 2),
        out_specs=VMEM,
        scratch_shapes=[
            pltpu.VMEM((total, width), BF16),
            pltpu.VMEM((total + 2 * WINDOW, kv_cols), BF16),
            pltpu.VMEM((kv_cols + 16, total + 2 * WINDOW), BF16),
            pltpu.VMEM((3, 3 * WINDOW, groups * WINDOW), F32),
        ],
        cost_estimate=cost(1.5e9, 3 << 20),
        compiler_params=PARAMS,
        name="attend",
    )(sink, *proj, low, high)


def totals_kernel(n_chunks, ret_local, n_sp, *refs):
    crow_ref = refs[0]
    sum_refs = refs[1 : 1 + n_chunks]
    out_ref = refs[-1]
    me = lax.axis_index("sp")
    last = crow_ref.shape[1] - 1
    line = lax.broadcasted_iota(jnp.int32, (EXTRA, RV), 0)
    for h in range(ret_local):
        sums = sum_refs[0][h]
        for ref in sum_refs[1:]:
            sums = sums + ref[h]
        end = jnp.broadcast_to(crow_ref[h : h + 1, last : last + 1], (EXTRA, RV))
        d0 = end.astype(BF16).astype(F32)
        d1 = (end - d0).astype(BF16).astype(F32)
        d2 = end - d0 - d1
        extra = jnp.where(line == 0, d0, jnp.where(line == 1, d1, jnp.where(line == 2, d2, 0.0)))
        fwd = jnp.concatenate([sums[:, :RV], extra], axis=0).astype(BF16)
        bwd = jnp.concatenate([sums[:, RV:], extra], axis=0).astype(BF16)
        for j in range(n_sp):
            out_ref[j, h] = jnp.where(j > me, fwd, bwd)


def totals(crow, sums, n_sp):
    ret_local = sums[0].shape[0]
    return pl.pallas_call(
        functools.partial(totals_kernel, len(sums), ret_local, n_sp),
        out_shape=jax.ShapeDtypeStruct((n_sp, ret_local, RK + EXTRA, RV), BF16),
        in_specs=[VMEM] * (1 + len(sums)),
        out_specs=VMEM,
        cost_estimate=cost(0.1e9, 1 << 20),
        compiler_params=PARAMS,
        name="totals",
    )(crow, *sums)


def local_kernel(n_chunks, ret_local, *refs):
    ccol_ref, crow_ref = refs[:2]
    proj = refs[2 : 2 + n_chunks]
    out_ref = refs[2 + n_chunks]
    qbuf, kbuf, vbuf = refs[-3:]
    total = crow_ref.shape[1]
    cols = ret_local * RK
    at = 0
    for ref in proj:
        here = pl.ds(at, ref.shape[1])
        qbuf[here] = ref[2, :, :cols]
        kbuf[here] = ref[2, :, cols:]
        vbuf[here] = ref[3]
        at += ref.shape[1]
    block = min(256, total)
    lane = lax.broadcasted_iota(jnp.int32, (block, cols), 1)

    def step(i, carry):
        here = pl.ds(pl.multiple_of(i * block, block), block)
        q = qbuf[here]
        for h in range(ret_local):
            mine = (lane >= h * RK) & (lane < (h + 1) * RK)
            qh = jnp.where(mine, q, jnp.zeros_like(q))
            gap = ccol_ref[here, h : h + 1] - crow_ref[h : h + 1, :]
            w = (dot_t(qh, kbuf[...]) * jnp.exp(-jnp.abs(gap))).astype(BF16)
            out_ref[here, h * RV : (h + 1) * RV] = dot(w, vbuf[:, h * RV : (h + 1) * RV])
        return carry

    lax.fori_loop(0, total // block, step, 0)


def local(ccol, crow, proj, ret_local):
    n = len(proj)
    width = proj[0].shape[2]
    total = crow.shape[1]
    return pl.pallas_call(
        functools.partial(local_kernel, n, ret_local),
        out_shape=jax.ShapeDtypeStruct((total, width), F32),
        in_specs=[VMEM] * (n + 2),
        out_specs=VMEM,
        scratch_shapes=[
            pltpu.VMEM((total, ret_local * RK), BF16),
            pltpu.VMEM((total, ret_local * RK), BF16),
            pltpu.VMEM((total, width), BF16),
        ],
        cost_estimate=cost(1e9, 3 << 20),
        compiler_params=PARAMS,
        name="local",
    )(ccol, crow, *proj)


def cross_kernel(n_chunks, ret_local, n_sp, *refs):
    crow_ref, ccol_ref, got_ref, init_ref, loc_ref = refs[:5]
    proj = refs[5 : 5 + n_chunks]
    out_ref, states = refs[-2:]
    me = lax.axis_index("sp")
    last = crow_ref.shape[1] - 1
    states[...] = jnp.zeros(states.shape, BF16)
    for h in range(ret_local):
        ends = []
        for j in range(n_sp):
            tail = got_ref[j, h, RK : RK + EXTRA, :].astype(F32)
            ends.append(jnp.sum(tail, axis=0, keepdims=True))
        for side, order in enumerate((range(n_sp - 1, -1, -1), range(n_sp))):
            state = jnp.zeros((RK, RV), F32)
            run = jnp.zeros((1, RV), F32)
            for j in order:
                here = (j < me) if side == 0 else (j > me)
                term = jnp.exp(run) * got_ref[j, h, 0:RK, :].astype(F32)
                state = state + jnp.where(here, term, 0.0)
                run = run + jnp.where(here, ends[j], 0.0)
            state = state + jnp.exp(run) * init_ref[side, h]
            col = (2 * h + side) * RV
            states[h * RK : (h + 1) * RK, col : col + RV] = state.astype(BF16)
    block = min(256, last + 1)
    first = 0
    for ref in proj:

        def step(i, carry, ref=ref, first=first):
            inner = pl.ds(pl.multiple_of(i * block, block), block)
            here = pl.ds(pl.multiple_of(first + i * block, block), block)
            both = dot(ref[2, inner, : ret_local * RK], states[...])
            for h in range(ret_local):
                col = ccol_ref[here, h : h + 1]
                ret = (
                    loc_ref[here, h * RV : (h + 1) * RV]
                    + jnp.exp(col) * both[:, 2 * h * RV : (2 * h + 1) * RV]
                    + jnp.exp(crow_ref[h : h + 1, last : last + 1] - col) * both[:, (2 * h + 1) * RV : (2 * h + 2) * RV]
                )
                centered = ret - jnp.mean(ret, axis=1, keepdims=True)
                scale = lax.rsqrt(jnp.mean(centered * centered, axis=1, keepdims=True) + NORM_EPS)
                gate = ref[4, inner, h * RV : (h + 1) * RV].astype(F32)
                gated = gate / (1.0 + jnp.exp(-gate))
                out_ref[here, h * RV : (h + 1) * RV] = (gated * (centered * scale)).astype(BF16)
            return carry

        lax.fori_loop(0, ref.shape[1] // block, step, 0)
        first += ref.shape[1]


def cross(crow, ccol, got, init, loc, proj, ret_local, n_sp):
    n = len(proj)
    width = proj[0].shape[2]
    total = crow.shape[1]
    return pl.pallas_call(
        functools.partial(cross_kernel, n, ret_local, n_sp),
        out_shape=jax.ShapeDtypeStruct((total, width), BF16),
        in_specs=[VMEM] * (n + 5),
        out_specs=VMEM,
        scratch_shapes=[pltpu.VMEM((ret_local * RK, 2 * ret_local * RV), BF16)],
        cost_estimate=cost(0.5e9, 4 << 20),
        compiler_params=PARAMS,
        name="cross",
    )(crow, ccol, got, init, loc, *proj)


def rows_of(ref, part, far, cols, core):
    share = ref.shape[2] // 2
    at = pl.ds(pl.multiple_of(core * cols, cols), cols)
    pieces = [ref[s, far, part * share : (part + 1) * share, at] for s in range(ref.shape[0])]
    return jnp.concatenate(pieces, axis=0)


def far_rows(spread, peer_spread, part, cols):
    core = lax.rem(lax.axis_index("tp"), 2)
    out = []
    for far in range(spread.shape[1]):
        out.append(rows_of(spread, part, far, cols, core))
        out.append(rows_of(peer_spread, part, far, cols, core))
    return out


def most_kernel(*refs):
    near_att, near_ret, peer_att, peer_ret, spread, peer_spread = refs[:6]
    data = refs[6:-1]
    out_ref = refs[-1]
    cols = out_ref.shape[1]
    mine = pl.ds(pl.multiple_of(lax.axis_index("tp") * cols, cols), cols)
    pieces = [near_att[:, mine], peer_att[:, mine]] + far_rows(spread, peer_spread, 0, cols)
    pieces += [near_ret[:, mine], peer_ret[:, mine]]
    right = jnp.concatenate(pieces, axis=0)
    rows = min(256, out_ref.shape[0])
    for i in range(out_ref.shape[0] // rows):
        here = pl.ds(i * rows, rows)
        out_ref[here] = dot(jnp.concatenate([ref[here] for ref in data], axis=1), right)


def last_kernel(*refs):
    spread, peer_spread, base = refs[:3]
    data = refs[3:-1]
    out_ref = refs[-1]
    right = jnp.concatenate(far_rows(spread, peer_spread, 1, out_ref.shape[1]), axis=0)
    rows = min(256, out_ref.shape[0])
    for i in range(out_ref.shape[0] // rows):
        here = pl.ds(i * rows, rows)
        part = dot(jnp.concatenate([ref[here] for ref in data], axis=1), right)
        out_ref[here] = (part + base[here]).astype(BF16)


def output(kernel, operands, shape, dtype):
    return pl.pallas_call(
        kernel,
        out_shape=jax.ShapeDtypeStruct(shape, dtype),
        in_specs=[VMEM] * len(operands),
        out_specs=VMEM,
        cost_estimate=cost(1e9, 8 << 20),
        compiler_params=PARAMS,
    )(*operands)


def core_swap(value):
    n = lax.axis_size("tp")
    return lax.ppermute(value, "tp", [(i, i ^ 1) for i in range(n)])


def chip_turn(value, by):
    n = lax.axis_size("tp")
    return lax.ppermute(value, "tp", [(i, (i + 2 * by) % n) for i in range(n)])


def gather_tp(value):
    blocks = [value, core_swap(value)]
    for by in range(1, lax.axis_size("tp") // 2):
        far = chip_turn(value, by)
        blocks += [far, core_swap(far)]
    return blocks


def sources():
    n = lax.axis_size("tp")
    me = lax.axis_index("tp")
    out = [me, me ^ 1]
    for by in range(1, n // 2):
        far = lax.rem(me + (n - 2 * by), n)
        out += [far, far ^ 1]
    return out


def output_weights(out_att, out_ret, slabs):
    n_sp = lax.axis_size("sp")
    moved = []
    for by, slab in enumerate(slabs, 1):
        moved.append(chip_turn(slab, by))
    spread = repeat(moved, n_sp)
    spread = lax.all_to_all(spread, "sp", 0, 0, tiled=True)
    share, cols = slabs[0].shape[0] // 2, slabs[0].shape[1]
    if share % 16:
        shape = (n_sp, len(slabs), 2, share, cols)
        spread = jnp.transpose(spread.reshape(shape), (1, 2, 0, 3, 4))
        spread = spread.reshape(1, len(slabs), -1, cols)
    peers = [core_swap(w) for w in (out_att, out_ret)]
    peer_spread = core_swap(spread)
    return [out_att, out_ret] + peers + [spread, peer_spread]


def body(
    tokens,
    norm_gain,
    att_query,
    att_key,
    att_value,
    ret_query,
    ret_key,
    ret_value,
    ret_gate,
    att_sink,
    decay_log,
    init_state,
    out_att,
    out_ret,
):
    n_sp = lax.axis_size("sp")
    total = tokens.shape[0]
    seq_len = total * n_sp
    width = att_query.shape[1]
    half = width // 2
    kv_local = att_key.shape[1] // HD
    groups = att_sink.shape[0] // kv_local
    ret_local = decay_log.shape[0]
    cols = tokens.shape[1]

    pieces, slabs = split(tokens, out_att, out_ret)
    near = core_swap(tokens)
    far = {}
    for c in ORDER:
        far[c] = []
        for by in range(1, lax.axis_size("tp") // 2):
            block = chip_turn(pieces[c], by)
            far[c] += [block, core_swap(block)]

    lane = np.arange(ret_local * RK)
    swap = np.zeros((lane.size, lane.size), np.float32)
    swap[lane ^ (RK // 2), lane] = np.where(lane % RK < RK // 2, -1.0, 1.0)
    swap = jnp.asarray(swap, BF16)
    mix = np.zeros((width, width), np.float32)
    for g in range(kv_local):
        for j in range(groups):
            for i in range(HD):
                mix[(g * groups + j) * HD + i, (j * kv_local + g) * HD + i] = 1.0
    mix = jnp.asarray(mix, BF16)
    crow, ccol, cos, sin = prepare(decay_log)

    if half % 128 == 0:
        weights = [att_query, att_key, att_value, ret_query, ret_key, ret_value, ret_gate]
        parts = [(0, 0), (1, 0), (1, half), (2, 0), (2, half), (3, 0), (4, 0)]
    else:
        weights = [
            att_query,
            jnp.concatenate([att_key, att_value], axis=1),
            jnp.concatenate([ret_query, ret_key], axis=1),
            ret_value,
            ret_gate,
        ]
        parts = [(i, 0) for i in range(5)]
    gain = norm_gain[None, :]
    out_w = output_weights(out_att, out_ret, slabs)
    proj = [None] * len(CHUNKS)
    sums = [None] * len(CHUNKS)
    edges = [None] * len(CHUNKS)
    for c in ORDER:
        first, rows = CHUNKS[c][0] * total // 4, CHUNKS[c][1] * total // 4
        proj[c], sums[c], *edges[c] = project(
            gain, crow, ccol, swap, mix, cos, sin, [tokens, near] + far[c], weights, parts,
            first, rows, ret_local,
        )

    forward = [(i, (i + 1) % n_sp) for i in range(n_sp)]
    backward = [(target, source) for source, target in forward]
    low = lax.ppermute(edges[-1][0], "sp", forward)
    high = lax.ppermute(edges[0][1], "sp", backward)

    sent = totals(crow, sums, n_sp)
    got = lax.all_to_all(sent, "sp", 0, 0, tiled=True)
    attended = attend(att_sink, proj, low, high, kv_local, groups, seq_len)
    att_blocks = gather_tp(attended)
    loc = local(ccol, crow, proj, ret_local)
    kept = cross(crow, ccol, got, init_state, loc, proj, ret_local, n_sp)
    ret_blocks = gather_tp(kept)
    operands = out_w + att_blocks + ret_blocks[:2]
    most = output(most_kernel, operands, (total, cols), F32)
    operands = out_w[4:] + [most] + ret_blocks[2:]
    return output(last_kernel, operands, (total, cols), BF16)


def solution(mesh):
    in_specs = (
        P("sp", "tp"),
        P(),
        P(None, "tp"),
        P(None, "tp"),
        P(None, "tp"),
        P(None, "tp"),
        P(None, "tp"),
        P(None, "tp"),
        P(None, "tp"),
        P("tp"),
        P("tp", "sp"),
        P(None, "tp", None, None),
        P("tp", None),
        P("tp", None),
    )
    out_specs = P("sp", "tp")
    return jax.shard_map(body, mesh=mesh, in_specs=in_specs, out_specs=out_specs, check_vma=False)
```

```python
import functools
import math

import jax
import jax.numpy as jnp
import numpy as np
from jax import lax
from jax.experimental import pallas as pl
from jax.experimental.pallas import tpu as pltpu
from jax.sharding import PartitionSpec as P


HD = 64
RK = 64
RV = 128
WINDOW = 128
NORM_EPS = 1e-06
ROPE_BASE = 10000.0
NEG = -1e30
EXTRA = 16
CHUNKS = ((0, 1), (1, 1), (2, 2))
ORDER = (2, 0, 1)
TABLE = 32
F32 = jnp.float32
BF16 = jnp.bfloat16

VMEM = pl.BlockSpec(memory_space=pltpu.VMEM)
SMEM = pl.BlockSpec(memory_space=pltpu.SMEM)
HBM = pl.BlockSpec(memory_space=pltpu.HBM)
PARAMS = pltpu.CompilerParams(vmem_limit_bytes=16 << 20)


def cost(flops, nbytes):
    return pl.CostEstimate(flops=int(flops), bytes_accessed=int(nbytes), transcendentals=0)


def dot(a, b):
    return jnp.dot(a, b, preferred_element_type=F32)


def dot_t(a, b):
    return lax.dot_general(a, b, (((1,), (1,)), ((), ())), preferred_element_type=F32)


def t_dot(a, b):
    return lax.dot_general(a, b, (((0,), (0,)), ((), ())), preferred_element_type=F32)


def in_vmem(values):
    return [pltpu.with_memory_space_constraint(v, pltpu.VMEM) for v in values]


def in_hbm(values):
    return [pltpu.with_memory_space_constraint(v, pltpu.HBM) for v in values]


class Copies:
    def __init__(self, sems):
        self.sems = sems
        self.copies = []

    def start(self, src, dst):
        copy = pltpu.make_async_copy(src, dst, self.sems.at[len(self.copies)])
        copy.start()
        self.copies.append(copy)

    def wait(self, first=0, last=None):
        for copy in self.copies[first:last]:
            copy.wait()


def slab_kernel(n_far, *refs):
    att, ret = refs[:2]
    slabs = refs[2 : 2 + n_far]
    copies = Copies(refs[-1])
    tp, sp = lax.axis_index("tp"), lax.axis_index("sp")
    chips = n_far + 1
    for by, slab in enumerate(slabs, 1):
        share, width = slab.shape[0] // 2, slab.shape[1]
        target = lax.rem(tp // 2 + by, chips)
        rows = pl.ds(pl.multiple_of(sp * share, share), share)
        cols = pl.ds(pl.multiple_of(target * width, width), width)
        for i, ref in enumerate((att, ret)):
            copies.start(ref.at[rows, cols], slab.at[pl.ds(i * share, share)])
    copies.wait()


def slab(att, ret, cols):
    chips = lax.axis_size("tp") // 2
    share = att.shape[0] // lax.axis_size("sp")
    if share % 16:
        rows = lax.axis_index("sp") * share
        out = []
        for by in range(1, chips):
            target = lax.rem(lax.axis_index("tp") // 2 + by, chips) * 2 * cols
            parts = [lax.dynamic_slice(w, (rows, target), (share, 2 * cols)) for w in (att, ret)]
            out.append(jnp.concatenate(parts, axis=0))
        return out
    return pl.pallas_call(
        functools.partial(slab_kernel, chips - 1),
        out_shape=(jax.ShapeDtypeStruct((2 * share, 2 * cols), BF16),) * (chips - 1),
        in_specs=[HBM, HBM],
        out_specs=(VMEM,) * (chips - 1),
        scratch_shapes=[pltpu.SemaphoreType.DMA((2 * chips,))],
        cost_estimate=cost(0.1e9, 3 << 20),
        compiler_params=PARAMS,
        name="slab",
    )(*in_hbm([att, ret]))


def split_kernel(n_pieces, *refs):
    tokens = refs[0]
    pieces = refs[1 : 1 + n_pieces]
    copies = Copies(refs[-1])
    for (first, _), piece in zip(CHUNKS, pieces):
        rows = pl.ds(first * tokens.shape[0] // 4, piece.shape[0])
        copies.start(tokens.at[rows], piece)
    copies.wait()


def split(tokens):
    total, cols = tokens.shape
    return pl.pallas_call(
        functools.partial(split_kernel, len(CHUNKS)),
        out_shape=tuple(jax.ShapeDtypeStruct((n * total // 4, cols), BF16) for _, n in CHUNKS),
        in_specs=[HBM],
        out_specs=(VMEM,) * len(CHUNKS),
        scratch_shapes=[pltpu.SemaphoreType.DMA((len(CHUNKS),))],
        cost_estimate=cost(0.1e9, 3 << 20),
        compiler_params=PARAMS,
        name="split",
    )(*in_hbm([tokens]))


def repeat_kernel(*refs):
    out_ref = refs[-1]
    for s in range(out_ref.shape[0]):
        for i, ref in enumerate(refs[:-1]):
            out_ref[s, i] = ref[...]


def repeat(slabs, count):
    return pl.pallas_call(
        repeat_kernel,
        out_shape=jax.ShapeDtypeStruct((count, len(slabs)) + slabs[0].shape, BF16),
        in_specs=[VMEM] * len(slabs),
        out_specs=VMEM,
        cost_estimate=cost(0.1e9, 1 << 20),
        compiler_params=PARAMS,
        name="repeat",
    )(*slabs)


def prepare_kernel(log_ref, *refs):
    row_ref, col_ref, cos_ref, sin_ref = refs[-4:]
    total = log_ref.shape[1]
    heads = log_ref.shape[0]
    sums = jnp.concatenate([log_ref[...], jnp.zeros((8 - heads, total), F32)], axis=0)
    lane = lax.broadcasted_iota(jnp.int32, sums.shape, 1)
    step = 1
    while step < total:
        sums = sums + jnp.where(lane >= step, pltpu.roll(sums, step, 1), 0.0)
        step *= 2
    row_ref[...] = sums
    col_ref[...] = sums.T
    rows, lanes = cos_ref.shape
    row = lax.broadcasted_iota(jnp.int32, (rows, lanes), 0)
    pair = lax.broadcasted_iota(jnp.int32, (rows, lanes), 1) & (RK // 2 - 1)
    count = total // TABLE
    place = jnp.where(row < count, lax.axis_index("sp") * total + TABLE * row, row - count)
    inverse = jnp.exp(pair.astype(F32) * (-2.0 * math.log(ROPE_BASE) / RK))
    angles = place.astype(F32) * inverse
    cos_ref[...] = jnp.cos(angles)
    sin_ref[...] = jnp.sin(angles)


def prepare(log, weights):
    heads, total = log.shape
    table = jax.ShapeDtypeStruct((total // TABLE + TABLE, heads * RK), F32)
    return pl.pallas_call(
        prepare_kernel,
        out_shape=(
            pltpu.VMEM((8, total), F32),
            pltpu.VMEM((total, 8), F32),
            table,
            table,
        ),
        in_specs=[VMEM] * (1 + len(weights)),
        out_specs=(VMEM,) * 4,
        cost_estimate=cost(8e9, 1 << 16),
        compiler_params=PARAMS,
        name="prepare",
    )(log, *weights)


def project_kernel(n_blocks, n_w, parts, first, ret_local, *refs):
    gain_ref, ccol_ref, swap_ref, mix_ref, cos_ref, sin_ref = refs[:6]
    blocks = refs[6 : 6 + n_blocks]
    w_refs = refs[6 + n_blocks : 6 + n_blocks + n_w]
    out_ref, sum_ref, low_ref, high_ref = refs[6 + n_blocks + n_w : 10 + n_blocks + n_w]
    xn, inv, held, sems = refs[-4:]
    copies = Copies(sems)
    width = blocks[0].shape[1]
    rows = xn.shape[0]
    group_width = inv.shape[1]
    half = group_width // 2
    total = ccol_ref.shape[0]
    mine = pl.ds(first, rows)
    starts = [pl.multiple_of(i * width, width) for i in sources()]
    tile = min(128, rows)
    lanes = min(128, width)
    for r in range(rows // tile):
        here = pl.ds(r * tile, tile)
        squares = jnp.zeros((tile, lanes), F32)
        for start, block in zip(starts, blocks):
            at = here if block.shape[0] == rows else pl.ds(first + r * tile, tile)
            for low in range(0, width, lanes):
                part = block[at, low : low + lanes].astype(F32)
                squares = squares + part * part
                col = pl.ds(pl.multiple_of(start + low, lanes), lanes)
                xn[here, col] = (part * gain_ref[:, col]).astype(BF16)
        mean = jnp.sum(squares, axis=1, keepdims=True) / (width * n_blocks)
        inv[here, :] = jnp.broadcast_to(lax.rsqrt(mean + NORM_EPS), (tile, group_width))
    count = total // TABLE
    cos_b, sin_b = cos_ref[count:], sin_ref[count:]
    cosines, sines = [], []
    for k in range(first // TABLE, (first + rows) // TABLE):
        cos_k, sin_k = cos_ref[k : k + 1], sin_ref[k : k + 1]
        cosines.append(cos_k * cos_b - sin_k * sin_b)
        sines.append(sin_k * cos_b + cos_k * sin_b)
    cosine = jnp.concatenate(cosines, axis=0)
    sine = jnp.concatenate(sines, axis=0)
    for group in (2, 3, 0, 1, 4):
        ws = [w[...] for w, (g, _) in zip(w_refs, parts) if g == group]
        w = ws[0] if len(ws) == 1 else jnp.concatenate(ws, axis=1)
        raw = (dot(xn[...], w) * inv[...]).astype(BF16)
        if group == 0:
            raw = (dot(raw, mix_ref[...]) * HD ** (-0.5)).astype(BF16)
        if group == 2:
            sides = []
            for low, scale in ((0, 1.0), (half, RK ** (-0.5))):
                side = raw[:, low : low + half]
                turned = side.astype(F32) * cosine + dot(side, swap_ref[...]) * sine
                sides.append((turned * scale).astype(BF16))
            keys = sides[1]
            raw = jnp.concatenate(sides, axis=1)
        if group == 3:
            for h in range(ret_local):
                col = ccol_ref[mine, h : h + 1]
                end = ccol_ref[total - 1 : total, h : h + 1]
                v = raw[:, h * RV : (h + 1) * RV].astype(F32)
                both = jnp.concatenate([v * jnp.exp(end - col), v * jnp.exp(col)], axis=1)
                sum_ref[h] = t_dot(keys, both.astype(BF16))[h * RK : (h + 1) * RK]
        if group == 1:
            low_ref[...] = raw[rows - WINDOW :]
            high_ref[...] = raw[:WINDOW]
        held[group] = raw
        copies.start(held.at[group], out_ref.at[group])
    copies.wait()


def project(gain, ccol, swap, mix, cos, sin, blocks, weights, parts, first, rows, ret_local):
    width = mix.shape[0]
    depth = gain.shape[1]
    n = len(blocks)
    return pl.pallas_call(
        functools.partial(project_kernel, n, len(weights), parts, first, ret_local),
        out_shape=(
            pltpu.HBM((5, rows, width), BF16),
            pltpu.VMEM((ret_local, RK, 2 * RV), F32),
            jax.ShapeDtypeStruct((WINDOW, width), BF16),
            jax.ShapeDtypeStruct((WINDOW, width), BF16),
        ),
        in_specs=[VMEM] * (n + 6 + len(weights)),
        out_specs=(HBM, VMEM, VMEM, VMEM),
        scratch_shapes=[
            pltpu.VMEM((rows, depth), BF16),
            pltpu.VMEM((rows, width), F32),
            pltpu.VMEM((5, rows, width), BF16),
            pltpu.SemaphoreType.DMA((5,)),
        ],
        cost_estimate=cost(2 * rows * depth * 5 * width // 4, 7 << 20),
        compiler_params=PARAMS,
        name="project",
    )(gain, ccol, swap, mix, cos, sin, *blocks, *weights)


def attend_kernel(n_chunks, kv_local, groups, seq_len, *refs):
    sink_ref = refs[0]
    proj = refs[1 : 1 + n_chunks]
    low_ref, high_ref, out_ref = refs[1 + n_chunks : 4 + n_chunks]
    qbuf, kvbuf, vbuf, mask, sems = refs[-5:]
    copies = Copies(sems)
    total = sum(ref.shape[1] for ref in proj)
    offset = lax.axis_index("sp") * total
    kv_cols = kv_local * HD
    block = WINDOW
    span = block + 2 * WINDOW
    copies.start(low_ref, kvbuf.at[pl.ds(0, WINDOW)])
    copies.start(high_ref, kvbuf.at[pl.ds(WINDOW + total, WINDOW)])
    for group, buf, at in ((1, kvbuf, WINDOW), (0, qbuf, 0)):
        for ref in proj:
            copies.start(ref.at[group], buf.at[pl.ds(at, ref.shape[1])])
            at += ref.shape[1]
    vbuf[kv_cols:] = jnp.ones((vbuf.shape[0] - kv_cols, vbuf.shape[1]), BF16)
    row = lax.broadcasted_iota(jnp.int32, (span, block), 1)
    col = lax.broadcasted_iota(jnp.int32, (span, block), 0)
    band = (col >= row) & (col <= row + 2 * WINDOW)
    for i, first in enumerate((0, block, total - block)):
        pos = col + (offset + first - WINDOW)
        allowed = band & (pos >= 0) & (pos < seq_len)
        one = jnp.where(allowed, 0.0, NEG)
        mask[i] = jnp.concatenate([one] * groups, axis=1)
    copies.wait()
    for i in range(kvbuf.shape[0] // block):
        here = pl.ds(i * block, block)
        vbuf[0:kv_cols, here] = kvbuf[here, kv_cols:].T
    lane = lax.broadcasted_iota(jnp.int32, (block, kv_cols), 1)
    n_steps = total // block

    def step(i, carry):
        first = pl.multiple_of(i * block, block)
        q = qbuf[pl.ds(first, block)]
        k = kvbuf[pl.ds(first, span), :kv_cols]
        kind = jnp.where(i == 0, 0, jnp.where(i == n_steps - 1, 2, 1))
        bias = mask[kind]
        scores = []
        for g in range(kv_local):
            mine = (lane >= g * HD) & (lane < (g + 1) * HD)
            tiles = []
            for j in range(groups):
                tile = q[:, j * kv_cols : (j + 1) * kv_cols]
                tiles.append(jnp.where(mine, tile, jnp.zeros_like(tile)))
            scores.append(dot_t(k, jnp.concatenate(tiles, axis=0)))
        weights = []
        rests = []
        for g in range(kv_local):
            s = scores[g] + bias
            sink = jnp.concatenate(
                [jnp.full((1, block), sink_ref[g * groups + j], F32) for j in range(groups)], axis=1
            )
            top = jnp.maximum(jnp.max(s, axis=0, keepdims=True), sink)
            weights.append(jnp.exp(s - top).astype(BF16))
            rests.append(jnp.exp(sink - top))
        outs = []
        for g in range(kv_local):
            v = vbuf[g * HD : (g + 1) * HD, pl.ds(first, span)]
            ones = vbuf[kv_cols : kv_cols + 16, pl.ds(first, span)]
            o = dot(jnp.concatenate([v, ones], axis=0), weights[g])
            o = o[:HD] / (o[HD : HD + 1] + rests[g])
            outs += [o[:, j * block : (j + 1) * block] for j in range(groups)]
        out_ref[pl.ds(first, block)] = jnp.concatenate(outs, axis=0).T.astype(BF16)
        return carry

    lax.fori_loop(0, n_steps, step, 0, unroll=n_steps)


def attend(sink, proj, low, high, kv_local, groups, seq_len):
    n = len(proj)
    width = proj[0].shape[2]
    total = sum(p.shape[1] for p in proj)
    kv_cols = kv_local * HD
    return pl.pallas_call(
        functools.partial(attend_kernel, n, kv_local, groups, seq_len),
        out_shape=jax.ShapeDtypeStruct((total, width), BF16),
        in_specs=[SMEM] + [HBM] * (n + 2),
        out_specs=VMEM,
        scratch_shapes=[
            pltpu.VMEM((total, width), BF16),
            pltpu.VMEM((total + 2 * WINDOW, 2 * kv_cols), BF16),
            pltpu.VMEM((kv_cols + 16, total + 2 * WINDOW), BF16),
            pltpu.VMEM((3, 3 * WINDOW, groups * WINDOW), F32),
            pltpu.SemaphoreType.DMA((2 * n + 2,)),
        ],
        cost_estimate=cost(1.5e9, 3 << 20),
        compiler_params=PARAMS,
        name="attend",
    )(sink, *in_hbm([*proj, low, high]))


def totals_kernel(n_chunks, ret_local, n_sp, *refs):
    ccol_ref = refs[0]
    sum_refs = refs[1 : 1 + n_chunks]
    out_ref = refs[-1]
    me = lax.axis_index("sp")
    last = ccol_ref.shape[0] - 1
    line = lax.broadcasted_iota(jnp.int32, (EXTRA, RV), 0)
    for h in range(ret_local):
        sums = sum_refs[0][h]
        for ref in sum_refs[1:]:
            sums = sums + ref[h]
        end = jnp.broadcast_to(ccol_ref[last : last + 1, h : h + 1], (EXTRA, RV))
        d0 = end.astype(BF16).astype(F32)
        d1 = (end - d0).astype(BF16).astype(F32)
        d2 = end - d0 - d1
        extra = jnp.where(line == 0, d0, jnp.where(line == 1, d1, jnp.where(line == 2, d2, 0.0)))
        fwd = jnp.concatenate([sums[:, :RV], extra], axis=0).astype(BF16)
        bwd = jnp.concatenate([sums[:, RV:], extra], axis=0).astype(BF16)
        for j in range(n_sp):
            out_ref[j, h] = jnp.where(j > me, fwd, bwd)


def totals(ccol, sums, n_sp):
    ret_local = sums[0].shape[0]
    return pl.pallas_call(
        functools.partial(totals_kernel, len(sums), ret_local, n_sp),
        out_shape=jax.ShapeDtypeStruct((n_sp, ret_local, RK + EXTRA, RV), BF16),
        in_specs=[VMEM] * (1 + len(sums)),
        out_specs=VMEM,
        cost_estimate=cost(0.1e9, 1 << 20),
        compiler_params=PARAMS,
        name="totals",
    )(ccol, *sums)


def local_kernel(n_chunks, ret_local, *refs):
    ccol_ref, crow_ref = refs[:2]
    proj = refs[2 : 2 + n_chunks]
    out_ref = refs[2 + n_chunks]
    rbuf, vbuf, sems = refs[-3:]
    total = crow_ref.shape[1]
    cols = ret_local * RK
    copies = Copies(sems)
    for group, buf in ((2, rbuf), (3, vbuf)):
        at = 0
        for ref in proj:
            copies.start(ref.at[group], buf.at[pl.ds(at, ref.shape[1])])
            at += ref.shape[1]
    copies.wait()
    block = min(256, total)
    lane = lax.broadcasted_iota(jnp.int32, (block, cols), 1)

    def step(i, carry):
        here = pl.ds(pl.multiple_of(i * block, block), block)
        q = rbuf[here, :cols]
        for h in range(ret_local):
            mine = (lane >= h * RK) & (lane < (h + 1) * RK)
            qh = jnp.where(mine, q, jnp.zeros_like(q))
            gap = ccol_ref[here, h : h + 1] - crow_ref[h : h + 1, :]
            w = (dot_t(qh, rbuf[:, cols:]) * jnp.exp(-jnp.abs(gap))).astype(BF16)
            out_ref[here, h * RV : (h + 1) * RV] = dot(w, vbuf[:, h * RV : (h + 1) * RV])
        return carry

    lax.fori_loop(0, total // block, step, 0)


def local(ccol, crow, proj, ret_local):
    n = len(proj)
    width = proj[0].shape[2]
    total = crow.shape[1]
    return pl.pallas_call(
        functools.partial(local_kernel, n, ret_local),
        out_shape=pltpu.VMEM((total, width), F32),
        in_specs=[VMEM, VMEM] + [HBM] * n,
        out_specs=VMEM,
        scratch_shapes=[
            pltpu.VMEM((total, width), BF16),
            pltpu.VMEM((total, width), BF16),
            pltpu.SemaphoreType.DMA((2 * n,)),
        ],
        cost_estimate=cost(1e9, 3 << 20),
        compiler_params=PARAMS,
        name="local",
    )(*in_vmem([ccol, crow]), *in_hbm(proj))


def cross_kernel(n_chunks, ret_local, n_sp, *refs):
    ccol_ref, loc_ref, got_hbm, init_hbm = refs[:4]
    proj = refs[4 : 4 + n_chunks]
    out_ref, states, got_ref, init_ref, qbuf, gbuf, sems = refs[-7:]
    me = lax.axis_index("sp")
    last = ccol_ref.shape[0] - 1
    copies = Copies(sems)
    copies.start(got_hbm, got_ref)
    copies.start(init_hbm, init_ref)
    for group, buf in ((2, qbuf), (4, gbuf)):
        at = 0
        for ref in proj:
            copies.start(ref.at[group], buf.at[pl.ds(at, ref.shape[1])])
            at += ref.shape[1]
    copies.wait(0, 2)
    states[...] = jnp.zeros(states.shape, BF16)
    for h in range(ret_local):
        ends = []
        for j in range(n_sp):
            tail = got_ref[j, h, RK : RK + EXTRA, :].astype(F32)
            ends.append(jnp.sum(tail, axis=0, keepdims=True))
        for side, order in enumerate((range(n_sp - 1, -1, -1), range(n_sp))):
            state = jnp.zeros((RK, RV), F32)
            run = jnp.zeros((1, RV), F32)
            for j in order:
                here = (j < me) if side == 0 else (j > me)
                term = jnp.exp(run) * got_ref[j, h, 0:RK, :].astype(F32)
                state = state + jnp.where(here, term, 0.0)
                run = run + jnp.where(here, ends[j], 0.0)
            state = state + jnp.exp(run) * init_ref[side, h]
            col = (2 * h + side) * RV
            states[h * RK : (h + 1) * RK, col : col + RV] = state.astype(BF16)
    copies.wait(2)
    block = min(256, last + 1)
    for i in range((last + 1) // block):
        here = pl.ds(i * block, block)
        both = dot(qbuf[here, : ret_local * RK], states[...])
        for h in range(ret_local):
            col = ccol_ref[here, h : h + 1]
            end = ccol_ref[last : last + 1, h : h + 1]
            ret = (
                loc_ref[here, h * RV : (h + 1) * RV]
                + jnp.exp(col) * both[:, 2 * h * RV : (2 * h + 1) * RV]
                + jnp.exp(end - col) * both[:, (2 * h + 1) * RV : (2 * h + 2) * RV]
            )
            centered = ret - jnp.mean(ret, axis=1, keepdims=True)
            scale = lax.rsqrt(jnp.mean(centered * centered, axis=1, keepdims=True) + NORM_EPS)
            gate = gbuf[here, h * RV : (h + 1) * RV].astype(F32)
            gated = gate / (1.0 + jnp.exp(-gate))
            out_ref[here, h * RV : (h + 1) * RV] = (gated * (centered * scale)).astype(BF16)


def cross(ccol, got, init, loc, proj, ret_local, n_sp):
    n = len(proj)
    width = proj[0].shape[2]
    total = ccol.shape[0]
    return pl.pallas_call(
        functools.partial(cross_kernel, n, ret_local, n_sp),
        out_shape=jax.ShapeDtypeStruct((total, width), BF16),
        in_specs=[VMEM, VMEM] + [HBM] * (n + 2),
        out_specs=VMEM,
        scratch_shapes=[
            pltpu.VMEM((ret_local * RK, 2 * ret_local * RV), BF16),
            pltpu.VMEM(got.shape, BF16),
            pltpu.VMEM(init.shape, F32),
            pltpu.VMEM((total, width), BF16),
            pltpu.VMEM((total, width), BF16),
            pltpu.SemaphoreType.DMA((2 * n + 2,)),
        ],
        cost_estimate=cost(0.5e9, 4 << 20),
        compiler_params=PARAMS,
        name="cross",
    )(*in_vmem([ccol, loc]), *in_hbm([got, init]), *in_vmem(proj))


def most_kernel(n_data, *refs):
    near_att, near_ret, peer_att, peer_ret, spread, peer_spread = refs[:6]
    data = refs[6 : 6 + n_data]
    out_ref, rest_ref = refs[6 + n_data : 8 + n_data]
    left, right, sems = refs[-3:]
    copies = Copies(sems)
    cols = out_ref.shape[1]
    tp = lax.axis_index("tp")
    mine = pl.ds(pl.multiple_of(tp * cols, cols), cols)
    half = pl.ds(pl.multiple_of(lax.rem(tp, 2) * cols, cols), cols)
    depth = near_att.shape[0]
    share = spread.shape[2] // 2
    at = 0
    for ref in (near_att, peer_att):
        copies.start(ref.at[:, mine], right.at[pl.ds(at, depth)])
        at += depth
    below = 0
    for far in range(spread.shape[1]):
        for ref in (spread, peer_spread):
            for s in range(spread.shape[0]):
                from_att = ref.at[s, far, pl.ds(0, share), half]
                from_ret = ref.at[s, far, pl.ds(share, share), half]
                copies.start(from_att, right.at[pl.ds(at + s * share, share)])
                copies.start(from_ret, rest_ref.at[pl.ds(below + s * share, share)])
            at += depth
            below += depth
    for ref in (near_ret, peer_ret):
        copies.start(ref.at[:, mine], right.at[pl.ds(at, depth)])
        at += depth
    for i, ref in enumerate(data):
        copies.start(ref, left.at[:, pl.ds(i * depth, depth)])
    copies.wait()
    rows = min(256, out_ref.shape[0])
    for i in range(out_ref.shape[0] // rows):
        here = pl.ds(i * rows, rows)
        out_ref[here] = dot(left[here], right[...])


def most(weights, data, cols):
    total, depth = data[0].shape
    n = len(data)
    spread = weights[4]
    count = 4 + 4 * spread.shape[0] * spread.shape[1] + n
    rest = 2 * spread.shape[1] * depth
    return pl.pallas_call(
        functools.partial(most_kernel, n),
        out_shape=(
            pltpu.VMEM((total, cols), F32),
            pltpu.VMEM((rest, cols), BF16),
        ),
        in_specs=[HBM] * (6 + n),
        out_specs=(VMEM, VMEM),
        scratch_shapes=[
            pltpu.VMEM((total, n * depth), BF16),
            pltpu.VMEM((n * depth, cols), BF16),
            pltpu.SemaphoreType.DMA((count,)),
        ],
        cost_estimate=cost(1e9, 8 << 20),
        compiler_params=PARAMS,
        name="most",
    )(*in_hbm(weights), *in_hbm(data))


def last_kernel(n_data, *refs):
    base, right = refs[:2]
    data = refs[2 : 2 + n_data]
    out_ref, held, sems = refs[-3:]
    copies = Copies(sems)
    rows = held.shape[1]
    for i in range(held.shape[0]):
        here = pl.ds(i * rows, rows)
        part = dot(jnp.concatenate([ref[here] for ref in data], axis=1), right[...])
        held[i] = (part + base[here]).astype(BF16)
        copies.start(held.at[i], out_ref.at[here])
    copies.wait()


def last(base, right, data):
    total, cols = base.shape
    rows = min(256, total)
    return pl.pallas_call(
        functools.partial(last_kernel, len(data)),
        out_shape=jax.ShapeDtypeStruct((total, cols), BF16),
        in_specs=[VMEM] * (2 + len(data)),
        out_specs=HBM,
        scratch_shapes=[
            pltpu.VMEM((total // rows, rows, cols), BF16),
            pltpu.SemaphoreType.DMA((total // rows,)),
        ],
        cost_estimate=cost(1e9, 8 << 20),
        compiler_params=PARAMS,
        name="last",
    )(*in_vmem([base, right]), *data)


def core_swap(value):
    n = lax.axis_size("tp")
    return lax.ppermute(value, "tp", [(i, i ^ 1) for i in range(n)])


def chip_turn(value, by):
    n = lax.axis_size("tp")
    return lax.ppermute(value, "tp", [(i, (i + 2 * by) % n) for i in range(n)])


def gather_tp(value):
    blocks = [value, core_swap(value)]
    for by in range(1, lax.axis_size("tp") // 2):
        far = chip_turn(value, by)
        blocks += [far, core_swap(far)]
    return blocks


def sources():
    n = lax.axis_size("tp")
    me = lax.axis_index("tp")
    out = [me, me ^ 1]
    for by in range(1, n // 2):
        far = lax.rem(me + (n - 2 * by), n)
        out += [far, far ^ 1]
    return out


def output_weights(out_att, out_ret, slabs):
    n_sp = lax.axis_size("sp")
    moved = []
    for by, slab in enumerate(slabs, 1):
        moved.append(chip_turn(slab, by))
    spread = repeat(moved, n_sp)
    spread = lax.all_to_all(spread, "sp", 0, 0, tiled=True)
    share, cols = slabs[0].shape[0] // 2, slabs[0].shape[1]
    if share % 16:
        shape = (n_sp, len(slabs), 2, share, cols)
        spread = jnp.transpose(spread.reshape(shape), (1, 2, 0, 3, 4))
        spread = spread.reshape(1, len(slabs), -1, cols)
    peers = [core_swap(w) for w in (out_att, out_ret)]
    peer_spread = core_swap(spread)
    return [out_att, out_ret] + peers + [spread, peer_spread]


def body(
    tokens,
    norm_gain,
    att_query,
    att_key,
    att_value,
    ret_query,
    ret_key,
    ret_value,
    ret_gate,
    att_sink,
    decay_log,
    init_state,
    out_att,
    out_ret,
):
    n_sp = lax.axis_size("sp")
    total = tokens.shape[0]
    seq_len = total * n_sp
    width = att_query.shape[1]
    half = width // 2
    kv_local = att_key.shape[1] // HD
    groups = att_sink.shape[0] // kv_local
    ret_local = decay_log.shape[0]
    cols = tokens.shape[1]

    slabs = slab(out_att, out_ret, cols)
    pieces = split(tokens)
    near = core_swap(tokens)
    far = {}
    for c in ORDER:
        far[c] = []
        for by in range(1, lax.axis_size("tp") // 2):
            block = chip_turn(pieces[c], by)
            far[c] += [block, core_swap(block)]

    lane = np.arange(ret_local * RK)
    swap = np.zeros((lane.size, lane.size), np.float32)
    swap[lane ^ (RK // 2), lane] = np.where(lane % RK < RK // 2, -1.0, 1.0)
    swap = jnp.asarray(swap, BF16)
    mix = np.zeros((width, width), np.float32)
    for g in range(kv_local):
        for j in range(groups):
            for i in range(HD):
                mix[(g * groups + j) * HD + i, (j * kv_local + g) * HD + i] = 1.0
    mix = jnp.asarray(mix, BF16)

    if half % 128 == 0:
        weights = [att_query, att_key, att_value, ret_query, ret_key, ret_value, ret_gate]
        parts = [(0, 0), (1, 0), (1, half), (2, 0), (2, half), (3, 0), (4, 0)]
    else:
        weights = [
            att_query,
            jnp.concatenate([att_key, att_value], axis=1),
            jnp.concatenate([ret_query, ret_key], axis=1),
            ret_value,
            ret_gate,
        ]
        parts = [(i, 0) for i in range(5)]
    gain = norm_gain[None, :]
    weights = in_vmem(weights)
    crow, ccol, cos, sin = prepare(decay_log, [])
    out_w = output_weights(out_att, out_ret, slabs)
    proj = [None] * len(CHUNKS)
    sums = [None] * len(CHUNKS)
    edges = [None] * len(CHUNKS)
    for c in ORDER:
        first, rows = CHUNKS[c][0] * total // 4, CHUNKS[c][1] * total // 4
        proj[c], sums[c], *edges[c] = project(
            gain, ccol, swap, mix, cos, sin, [tokens, near] + far[c], weights, parts,
            first, rows, ret_local,
        )

    forward = [(i, (i + 1) % n_sp) for i in range(n_sp)]
    backward = [(target, source) for source, target in forward]
    low = lax.ppermute(edges[-1][0], "sp", forward)
    high = lax.ppermute(edges[0][1], "sp", backward)

    sent = totals(ccol, sums, n_sp)
    got = lax.all_to_all(sent, "sp", 0, 0, tiled=True)
    attended = attend(att_sink, proj, low, high, kv_local, groups, seq_len)
    att_blocks = gather_tp(attended)
    loc = local(ccol, crow, proj, ret_local)
    kept = cross(ccol, got, init_state, loc, proj, ret_local, n_sp)
    ret_blocks = gather_tp(kept)
    base, right = most(out_w, att_blocks + ret_blocks[:2], cols)
    return last(base, right, ret_blocks[2:])


def solution(mesh):
    in_specs = (
        P("sp", "tp"),
        P(),
        P(None, "tp"),
        P(None, "tp"),
        P(None, "tp"),
        P(None, "tp"),
        P(None, "tp"),
        P(None, "tp"),
        P(None, "tp"),
        P("tp"),
        P("tp", "sp"),
        P(None, "tp", None, None),
        P("tp", None),
        P("tp", None),
    )
    out_specs = P("sp", "tp")
    return jax.shard_map(body, mesh=mesh, in_specs=in_specs, out_specs=out_specs, check_vma=False)
```

```python
import functools
import math

import jax
import jax.numpy as jnp
import numpy as np
from jax import lax
from jax.experimental import pallas as pl
from jax.experimental.pallas import tpu as pltpu
from jax.sharding import PartitionSpec as P


HD = 64
RK = 64
RV = 128
WINDOW = 128
NORM_EPS = 1e-06
ROPE_BASE = 10000.0
NEG = -1e30
EXTRA = 16
CHUNKS = ((0, 2), (2, 3), (5, 3))
ORDER = (2, 0, 1)
TABLE = 32
HALVES = 2
F32 = jnp.float32
BF16 = jnp.bfloat16

VMEM = pl.BlockSpec(memory_space=pltpu.VMEM)
SMEM = pl.BlockSpec(memory_space=pltpu.SMEM)
HBM = pl.BlockSpec(memory_space=pltpu.HBM)
PARAMS = pltpu.CompilerParams(vmem_limit_bytes=16 << 20)


def cost(flops, nbytes):
    return pl.CostEstimate(flops=int(flops), bytes_accessed=int(nbytes), transcendentals=0)


def dot(a, b):
    return jnp.dot(a, b, preferred_element_type=F32)


def dot_t(a, b):
    return lax.dot_general(a, b, (((1,), (1,)), ((), ())), preferred_element_type=F32)


def t_dot(a, b):
    return lax.dot_general(a, b, (((0,), (0,)), ((), ())), preferred_element_type=F32)


def in_vmem(values):
    return [pltpu.with_memory_space_constraint(v, pltpu.VMEM) for v in values]


def in_hbm(values):
    return [pltpu.with_memory_space_constraint(v, pltpu.HBM) for v in values]


class Copies:
    def __init__(self, sems):
        self.sems = sems
        self.copies = []

    def start(self, src, dst):
        copy = pltpu.make_async_copy(src, dst, self.sems.at[len(self.copies)])
        copy.start()
        self.copies.append(copy)

    def wait(self, first=0, last=None):
        for copy in self.copies[first:last]:
            copy.wait()


def slab_kernel(chips, *refs):
    weights = refs[:2]
    slabs = refs[2:-1]
    copies = Copies(refs[-1])
    tp = lax.axis_index("tp")
    for i, slab in enumerate(slabs):
        target = lax.rem(tp // 2 + 1 + i // 2, chips)
        width = slab.shape[1]
        cols = pl.ds(pl.multiple_of(target * width, width), width)
        copies.start(weights[i % 2].at[:, cols], slab)
    copies.wait()


def slab(att, ret, cols):
    chips = lax.axis_size("tp") // 2
    shape = jax.ShapeDtypeStruct((att.shape[0], 2 * cols), BF16)
    return pl.pallas_call(
        functools.partial(slab_kernel, chips),
        out_shape=(shape,) * (2 * chips - 2),
        in_specs=[HBM, HBM],
        out_specs=(VMEM,) * (2 * chips - 2),
        scratch_shapes=[pltpu.SemaphoreType.DMA((2 * chips - 2,))],
        cost_estimate=cost(0.1e9, 3 << 20),
        compiler_params=PARAMS,
        name="slab",
    )(*in_hbm([att, ret]))


def split_kernel(chunks, *refs):
    tokens = refs[0]
    pieces = refs[1 : 1 + len(chunks)]
    copies = Copies(refs[-1])
    for (first, _), piece in zip(chunks, pieces):
        rows = pl.ds(first * tokens.shape[0] // 8, piece.shape[0])
        copies.start(tokens.at[rows], piece)
    copies.wait()


def split(tokens, chunks):
    total, cols = tokens.shape
    return pl.pallas_call(
        functools.partial(split_kernel, chunks),
        out_shape=tuple(jax.ShapeDtypeStruct((n * total // 8, cols), BF16) for _, n in chunks),
        in_specs=[HBM],
        out_specs=(VMEM,) * len(chunks),
        scratch_shapes=[pltpu.SemaphoreType.DMA((len(chunks),))],
        cost_estimate=cost(0.1e9, 3 << 20),
        compiler_params=PARAMS,
        name="split",
    )(*in_hbm([tokens]))


def prepare_kernel(log_ref, *refs):
    row_ref, col_ref, cos_ref, sin_ref = refs[-4:]
    total = log_ref.shape[1]
    heads = log_ref.shape[0]
    sums = jnp.concatenate([log_ref[...], jnp.zeros((8 - heads, total), F32)], axis=0)
    lane = lax.broadcasted_iota(jnp.int32, sums.shape, 1)
    step = 1
    while step < total:
        sums = sums + jnp.where(lane >= step, pltpu.roll(sums, step, 1), 0.0)
        step *= 2
    row_ref[...] = sums
    col_ref[...] = sums.T
    rows, lanes = cos_ref.shape
    row = lax.broadcasted_iota(jnp.int32, (rows, lanes), 0)
    pair = lax.broadcasted_iota(jnp.int32, (rows, lanes), 1) & (RK // 2 - 1)
    count = total // TABLE
    place = jnp.where(row < count, lax.axis_index("sp") * total + TABLE * row, row - count)
    inverse = jnp.exp(pair.astype(F32) * (-2.0 * math.log(ROPE_BASE) / RK))
    angles = place.astype(F32) * inverse
    cos_ref[...] = jnp.cos(angles)
    sin_ref[...] = jnp.sin(angles)


def prepare(log, weights):
    heads, total = log.shape
    table = jax.ShapeDtypeStruct((total // TABLE + TABLE, heads * RK), F32)
    return pl.pallas_call(
        prepare_kernel,
        out_shape=(
            jax.ShapeDtypeStruct((8, total), F32),
            jax.ShapeDtypeStruct((total, 8), F32),
            table,
            table,
        ),
        in_specs=[VMEM] * (1 + len(weights)),
        out_specs=(VMEM,) * 4,
        cost_estimate=cost(8e9, 1 << 16),
        compiler_params=PARAMS,
        name="prepare",
    )(log, *weights)


def project_kernel(n_blocks, n_w, n_other, parts, first, ret_local, *refs):
    gain_ref, ccol_ref, swap_ref, mix_ref, cos_ref, sin_ref = refs[:6]
    blocks = refs[6 : 6 + n_blocks]
    w_refs = refs[6 + n_blocks : 6 + n_blocks + n_w]
    other_refs = refs[6 + n_blocks + n_w : 6 + n_blocks + n_w + n_other]
    at_out = 6 + n_blocks + n_w + n_other
    out_ref, sum_ref, low_ref, high_ref = refs[at_out : at_out + 4]
    xn, inv, held, sems = refs[-4:]
    copies = Copies(sems)
    width = blocks[0].shape[1]
    rows = xn.shape[0]
    group_width = inv.shape[1]
    half = group_width // 2
    total = ccol_ref.shape[0]
    mine = pl.ds(first, rows)
    starts = [pl.multiple_of(i * width, width) for i in sources()]
    tile = min(128, rows)
    lanes = min(128, width)
    for r in range(rows // tile):
        here = pl.ds(r * tile, tile)
        squares = jnp.zeros((tile, lanes), F32)
        for start, block in zip(starts, blocks):
            at = here if block.shape[0] == rows else pl.ds(first + r * tile, tile)
            for low in range(0, width, lanes):
                part = block[at, low : low + lanes].astype(F32)
                squares = squares + part * part
                col = pl.ds(pl.multiple_of(start + low, lanes), lanes)
                xn[here, col] = (part * gain_ref[:, col]).astype(BF16)
        mean = jnp.sum(squares, axis=1, keepdims=True) / (width * n_blocks)
        inv[here, :] = jnp.broadcast_to(lax.rsqrt(mean + NORM_EPS), (tile, group_width))
    count = total // TABLE
    cos_b, sin_b = cos_ref[count:], sin_ref[count:]
    cosines, sines = [], []
    for k in range(first // TABLE, (first + rows) // TABLE):
        cos_k, sin_k = cos_ref[k : k + 1], sin_ref[k : k + 1]
        cosines.append(cos_k * cos_b - sin_k * sin_b)
        sines.append(sin_k * cos_b + cos_k * sin_b)
    cosine = jnp.concatenate(cosines, axis=0)
    sine = jnp.concatenate(sines, axis=0)
    for group in (2, 3, 0, 1, 4):
        ws = [w[...] for w, (g, _) in zip(w_refs, parts) if g == group]
        w = ws[0] if len(ws) == 1 else jnp.concatenate(ws, axis=1)
        raw = (dot(xn[...], w) * inv[...]).astype(BF16)
        if group == 0:
            raw = (dot(raw, mix_ref[...]) * HD ** (-0.5)).astype(BF16)
        if group == 2:
            sides = []
            for low, scale in ((0, 1.0), (half, RK ** (-0.5))):
                side = raw[:, low : low + half]
                turned = side.astype(F32) * cosine + dot(side, swap_ref[...]) * sine
                sides.append((turned * scale).astype(BF16))
            keys = sides[1]
            raw = jnp.concatenate(sides, axis=1)
        if group == 3:
            for h in range(ret_local):
                col = ccol_ref[mine, h : h + 1]
                end = ccol_ref[total - 1 : total, h : h + 1]
                v = raw[:, h * RV : (h + 1) * RV].astype(F32)
                both = jnp.concatenate([v * jnp.exp(end - col), v * jnp.exp(col)], axis=1)
                sum_ref[h] = t_dot(keys, both.astype(BF16))[h * RK : (h + 1) * RK]
        if group == 1:
            low_ref[...] = raw[rows - WINDOW :]
            high_ref[...] = raw[:WINDOW]
            for other in other_refs:
                even = lax.rem(lax.axis_index("sp"), 2) == 0
                low_ref[...] = jnp.where(even, other[...], raw[:WINDOW])
                high_ref[...] = jnp.where(even, raw[:WINDOW], other[...])
        held[group] = raw
        copies.start(held.at[group], out_ref.at[group])
    copies.wait()


def project(gain, ccol, swap, mix, cos, sin, blocks, weights, parts, first, rows, ret_local, other):
    width = mix.shape[0]
    depth = gain.shape[1]
    n = len(blocks)
    return pl.pallas_call(
        functools.partial(project_kernel, n, len(weights), len(other), parts, first, ret_local),
        out_shape=(
            pltpu.HBM((5, rows, width), BF16),
            pltpu.VMEM((ret_local, RK, 2 * RV), F32),
            jax.ShapeDtypeStruct((WINDOW, width), BF16),
            jax.ShapeDtypeStruct((WINDOW, width), BF16),
        ),
        in_specs=[VMEM] * (n + 6 + len(weights) + len(other)),
        out_specs=(HBM, VMEM, VMEM, VMEM),
        scratch_shapes=[
            pltpu.VMEM((rows, depth), BF16),
            pltpu.VMEM((rows, width), F32),
            pltpu.VMEM((5, rows, width), BF16),
            pltpu.SemaphoreType.DMA((5,)),
        ],
        cost_estimate=cost(2 * rows * depth * 5 * width // 4, 7 << 20),
        compiler_params=PARAMS,
        name="project",
    )(gain, ccol, swap, mix, cos, sin, *blocks, *weights, *other)


def overlaps(sizes, first, rows):
    out = []
    at = 0
    for i, size in enumerate(sizes):
        low, high = max(at, first), min(at + size, first + rows)
        if low < high:
            out.append((i, low - at, high - low, low - first))
        at += size
    return out


def attend_kernel(n_chunks, kv_local, groups, seq_len, total, start, *refs):
    sink_ref = refs[0]
    proj = refs[1 : 1 + n_chunks]
    low_ref, high_ref, out_ref = refs[1 + n_chunks : 4 + n_chunks]
    qbuf, kvbuf, vbuf, mask, sems = refs[-5:]
    copies = Copies(sems)
    rows = out_ref.shape[0]
    offset = lax.axis_index("sp") * total
    kv_cols = kv_local * HD
    block = WINDOW
    span = block + 2 * WINDOW
    sizes = [WINDOW] + [ref.shape[1] for ref in proj] + [WINDOW]
    for i, low, count, to in overlaps(sizes, start, rows + 2 * WINDOW):
        if i in (0, n_chunks + 1):
            even = lax.rem(lax.axis_index("sp"), 2) == 0
            here = pl.ds(low, count)
            near, far = (high_ref, low_ref) if i == 0 else (low_ref, high_ref)
            kvbuf[pl.ds(to, count)] = jnp.where(even, near[here], far[here])
        else:
            copies.start(proj[i - 1].at[1, pl.ds(low, count)], kvbuf.at[pl.ds(to, count)])
    n_kv = len(copies.copies)
    for i, low, count, to in overlaps(sizes[1:-1], start, rows):
        copies.start(proj[i].at[0, pl.ds(low, count)], qbuf.at[pl.ds(to, count)])
    vbuf[kv_cols:] = jnp.ones((vbuf.shape[0] - kv_cols, vbuf.shape[1]), BF16)
    row = lax.broadcasted_iota(jnp.int32, (span, block), 1)
    col = lax.broadcasted_iota(jnp.int32, (span, block), 0)
    band = (col >= row) & (col <= row + 2 * WINDOW)
    n_steps = rows // block
    edges = [i for i in range(n_steps) if start + i * block in (0, total - block)]
    inner = jnp.where(band, 0.0, NEG)
    mask[0] = jnp.concatenate([inner] * groups, axis=1)
    for kind, i in enumerate(edges, 1):
        pos = col + (offset + start + i * block - WINDOW)
        one = jnp.where((pos >= 0) & (pos < seq_len), inner, NEG)
        mask[kind] = jnp.concatenate([one] * groups, axis=1)
    copies.wait(0, n_kv)
    for i in range(kvbuf.shape[0] // block):
        here = pl.ds(i * block, block)
        vbuf[0:kv_cols, here] = kvbuf[here, kv_cols:].T
    copies.wait(n_kv)
    lane = lax.broadcasted_iota(jnp.int32, (block, kv_cols), 1)
    for i in range(n_steps):
        first = i * block
        q = qbuf[pl.ds(first, block)]
        k = kvbuf[pl.ds(first, span), :kv_cols]
        bias = mask[edges.index(i) + 1 if i in edges else 0]
        scores = []
        for g in range(kv_local):
            mine = (lane >= g * HD) & (lane < (g + 1) * HD)
            tiles = []
            for j in range(groups):
                tile = q[:, j * kv_cols : (j + 1) * kv_cols]
                tiles.append(jnp.where(mine, tile, jnp.zeros_like(tile)))
            scores.append(dot_t(k, jnp.concatenate(tiles, axis=0)))
        weights = []
        rests = []
        for g in range(kv_local):
            s = scores[g] + bias
            sink = jnp.concatenate(
                [jnp.full((1, block), sink_ref[g * groups + j], F32) for j in range(groups)], axis=1
            )
            top = jnp.maximum(jnp.max(s, axis=0, keepdims=True), sink)
            weights.append(jnp.exp(s - top).astype(BF16))
            rests.append(jnp.exp(sink - top))
        outs = []
        for g in range(kv_local):
            v = vbuf[g * HD : (g + 1) * HD, pl.ds(first, span)]
            ones = vbuf[kv_cols : kv_cols + 16, pl.ds(first, span)]
            o = dot(jnp.concatenate([v, ones], axis=0), weights[g])
            o = o[:HD] / (o[HD : HD + 1] + rests[g])
            outs += [o[:, j * block : (j + 1) * block] for j in range(groups)]
        out_ref[pl.ds(first, block)] = jnp.concatenate(outs, axis=0).T.astype(BF16)


def attend(sink, proj, low, high, kv_local, groups, seq_len, start, rows):
    n = len(proj)
    width = proj[0].shape[2]
    total = sum(p.shape[1] for p in proj)
    kv_cols = kv_local * HD
    return pl.pallas_call(
        functools.partial(attend_kernel, n, kv_local, groups, seq_len, total, start),
        out_shape=jax.ShapeDtypeStruct((rows, width), BF16),
        in_specs=[SMEM] + [HBM] * n + [VMEM, VMEM],
        out_specs=VMEM,
        scratch_shapes=[
            pltpu.VMEM((rows, width), BF16),
            pltpu.VMEM((rows + 2 * WINDOW, 2 * kv_cols), BF16),
            pltpu.VMEM((kv_cols + 16, rows + 2 * WINDOW), BF16),
            pltpu.VMEM((3, 3 * WINDOW, groups * WINDOW), F32),
            pltpu.SemaphoreType.DMA((2 * n + 2,)),
        ],
        cost_estimate=cost(0.8e9, 3 << 20),
        compiler_params=PARAMS,
        name="attend",
    )(sink, *in_hbm(proj), low, high)


def totals_kernel(n_chunks, ret_local, n_sp, *refs):
    ccol_ref = refs[0]
    sum_refs = refs[1 : 1 + n_chunks]
    out_ref = refs[-1]
    me = lax.axis_index("sp")
    last = ccol_ref.shape[0] - 1
    line = lax.broadcasted_iota(jnp.int32, (EXTRA, RV), 0)
    for h in range(ret_local):
        sums = sum_refs[0][h]
        for ref in sum_refs[1:]:
            sums = sums + ref[h]
        end = jnp.broadcast_to(ccol_ref[last : last + 1, h : h + 1], (EXTRA, RV))
        d0 = end.astype(BF16).astype(F32)
        d1 = (end - d0).astype(BF16).astype(F32)
        d2 = end - d0 - d1
        extra = jnp.where(line == 0, d0, jnp.where(line == 1, d1, jnp.where(line == 2, d2, 0.0)))
        fwd = jnp.concatenate([sums[:, :RV], extra], axis=0).astype(BF16)
        bwd = jnp.concatenate([sums[:, RV:], extra], axis=0).astype(BF16)
        for j in range(n_sp):
            out_ref[j, h] = jnp.where(j > me, fwd, bwd)


def totals(ccol, sums, n_sp):
    ret_local = sums[0].shape[0]
    return pl.pallas_call(
        functools.partial(totals_kernel, len(sums), ret_local, n_sp),
        out_shape=jax.ShapeDtypeStruct((n_sp, ret_local, RK + EXTRA, RV), BF16),
        in_specs=[VMEM] * (1 + len(sums)),
        out_specs=VMEM,
        cost_estimate=cost(0.1e9, 1 << 20),
        compiler_params=PARAMS,
        name="totals",
    )(ccol, *sums)


def retain_kernel(n_chunks, ret_local, n_sp, *refs):
    ccol_hbm, crow_hbm, got_hbm, init_hbm = refs[:4]
    proj = refs[4 : 4 + n_chunks]
    outs = refs[4 + n_chunks : 4 + n_chunks + HALVES]
    states, got_ref, init_ref, ccol_ref, crow_ref, rbuf, vbuf, gbuf, sems = refs[-9:]
    me = lax.axis_index("sp")
    total = ccol_ref.shape[0]
    last = total - 1
    cols = ret_local * RK
    copies = Copies(sems)
    copies.start(got_hbm, got_ref)
    copies.start(init_hbm, init_ref)
    copies.start(ccol_hbm, ccol_ref)
    copies.start(crow_hbm, crow_ref)
    for group, buf in ((2, rbuf), (3, vbuf), (4, gbuf)):
        at = 0
        for ref in proj:
            copies.start(ref.at[group], buf.at[pl.ds(at, ref.shape[1])])
            at += ref.shape[1]
    copies.wait(0, 2)
    states[...] = jnp.zeros(states.shape, BF16)
    for h in range(ret_local):
        ends = []
        for j in range(n_sp):
            tail = got_ref[j, h, RK : RK + EXTRA, :].astype(F32)
            ends.append(jnp.sum(tail, axis=0, keepdims=True))
        for side, order in enumerate((range(n_sp - 1, -1, -1), range(n_sp))):
            state = jnp.zeros((RK, RV), F32)
            run = jnp.zeros((1, RV), F32)
            for j in order:
                here = (j < me) if side == 0 else (j > me)
                term = jnp.exp(run) * got_ref[j, h, 0:RK, :].astype(F32)
                state = state + jnp.where(here, term, 0.0)
                run = run + jnp.where(here, ends[j], 0.0)
            state = state + jnp.exp(run) * init_ref[side, h]
            col = (2 * h + side) * RV
            states[h * RK : (h + 1) * RK, col : col + RV] = state.astype(BF16)
    copies.wait(2)
    block = min(256, total // HALVES)
    lane = lax.broadcasted_iota(jnp.int32, (block, cols), 1)
    for i in range(total // block):
        here = pl.ds(i * block, block)
        out_ref = outs[i * block * HALVES // total]
        there = pl.ds(i * block % (total // HALVES), block)
        q = rbuf[here, :cols]
        both = dot(q, states[...])
        for h in range(ret_local):
            mine = (lane >= h * RK) & (lane < (h + 1) * RK)
            qh = jnp.where(mine, q, jnp.zeros_like(q))
            col = ccol_ref[here, h : h + 1]
            end = ccol_ref[last : last + 1, h : h + 1]
            gap = col - crow_ref[h : h + 1, :]
            w = (dot_t(qh, rbuf[:, cols:]) * jnp.exp(-jnp.abs(gap))).astype(BF16)
            ret = (
                dot(w, vbuf[:, h * RV : (h + 1) * RV])
                + jnp.exp(col) * both[:, 2 * h * RV : (2 * h + 1) * RV]
                + jnp.exp(end - col) * both[:, (2 * h + 1) * RV : (2 * h + 2) * RV]
            )
            centered = ret - jnp.mean(ret, axis=1, keepdims=True)
            scale = lax.rsqrt(jnp.mean(centered * centered, axis=1, keepdims=True) + NORM_EPS)
            gate = gbuf[here, h * RV : (h + 1) * RV].astype(F32)
            gated = gate / (1.0 + jnp.exp(-gate))
            out_ref[there, h * RV : (h + 1) * RV] = (gated * (centered * scale)).astype(BF16)


def retain(ccol, crow, got, init, proj, ret_local, n_sp):
    n = len(proj)
    width = proj[0].shape[2]
    total = ccol.shape[0]
    return pl.pallas_call(
        functools.partial(retain_kernel, n, ret_local, n_sp),
        out_shape=(jax.ShapeDtypeStruct((total // HALVES, width), BF16),) * HALVES,
        in_specs=[HBM] * (n + 4),
        out_specs=(VMEM,) * HALVES,
        scratch_shapes=[
            pltpu.VMEM((ret_local * RK, 2 * ret_local * RV), BF16),
            pltpu.VMEM(got.shape, BF16),
            pltpu.VMEM(init.shape, F32),
            pltpu.VMEM(ccol.shape, F32),
            pltpu.VMEM(crow.shape, F32),
            pltpu.VMEM((total, width), BF16),
            pltpu.VMEM((total, width), BF16),
            pltpu.VMEM((total, width), BF16),
            pltpu.SemaphoreType.DMA((3 * n + 4,)),
        ],
        cost_estimate=cost(1.5e9, 4 << 20),
        compiler_params=PARAMS,
        name="retain",
    )(*in_hbm([ccol, crow, got, init, *proj]))


def most_kernel(n_far, n_data, *refs):
    near_att, near_ret, peer_att, peer_ret = refs[:4]
    far_att, far_ret = refs[4 : 4 + n_far], refs[4 + n_far : 4 + 2 * n_far]
    data = refs[4 + 2 * n_far : 4 + 2 * n_far + n_data]
    out_ref, rest_ref = refs[4 + 2 * n_far + n_data : 6 + 2 * n_far + n_data]
    left, right, sems = refs[-3:]
    copies = Copies(sems)
    cols = out_ref.shape[1]
    tp = lax.axis_index("tp")
    mine = pl.ds(pl.multiple_of(tp * cols, cols), cols)
    half = pl.ds(pl.multiple_of(lax.rem(tp, 2) * cols, cols), cols)
    depth = near_att.shape[0]
    rows = [(ref, mine) for ref in (near_att, peer_att)] + [(ref, half) for ref in far_att]
    rows += [(ref, mine) for ref in (near_ret, peer_ret)]
    for i, (ref, at) in enumerate(rows):
        copies.start(ref.at[:, at], right.at[pl.ds(i * depth, depth)])
    for i, ref in enumerate(data):
        half_rows = pl.ds(i % HALVES * ref.shape[0], ref.shape[0])
        copies.start(ref, left.at[half_rows, pl.ds(i // HALVES * depth, depth)])
    for i, ref in enumerate(far_ret):
        copies.start(ref.at[:, half], rest_ref.at[pl.ds(i * depth, depth)])
    copies.wait()
    rows = min(256, out_ref.shape[0])
    for i in range(out_ref.shape[0] // rows):
        here = pl.ds(i * rows, rows)
        out_ref[here] = dot(left[here], right[...])


def most(weights, data, cols):
    total, depth = data[0].shape[0] * HALVES, data[0].shape[1]
    n = len(data)
    n_far = (len(weights) - 4) // 2
    return pl.pallas_call(
        functools.partial(most_kernel, n_far, n),
        out_shape=(
            pltpu.VMEM((total, cols), F32),
            pltpu.VMEM((n_far * depth, cols), BF16),
        ),
        in_specs=[HBM] * (len(weights) + n),
        out_specs=(VMEM, VMEM),
        scratch_shapes=[
            pltpu.VMEM((total, n // HALVES * depth), BF16),
            pltpu.VMEM((n // HALVES * depth, cols), BF16),
            pltpu.SemaphoreType.DMA((len(weights) + n,)),
        ],
        cost_estimate=cost(1e9, 8 << 20),
        compiler_params=PARAMS,
        name="most",
    )(*in_hbm(weights), *in_hbm(data))


def last_kernel(n_data, start, *refs):
    base, right = refs[:2]
    data = refs[2 : 2 + n_data]
    out_ref, held, sems = refs[-3:]
    copies = Copies(sems)
    rows = held.shape[1]
    for i in range(held.shape[0]):
        here = pl.ds(i * rows, rows)
        there = pl.ds(start + i * rows, rows)
        part = dot(jnp.concatenate([ref[here] for ref in data], axis=1), right[...])
        held[i] = (part + base[there]).astype(BF16)
        copies.start(held.at[i], out_ref.at[there])
    copies.wait()


def last(base, right, data, start, done):
    total, cols = base.shape
    part = data[0].shape[0]
    rows = min(256, part)
    n = len(data)
    extra = [] if done is None else [done]
    return pl.pallas_call(
        functools.partial(last_kernel, n, start),
        out_shape=jax.ShapeDtypeStruct((total, cols), BF16),
        in_specs=[VMEM] * (2 + n) + [HBM] * len(extra),
        out_specs=HBM,
        scratch_shapes=[
            pltpu.VMEM((part // rows, rows, cols), BF16),
            pltpu.SemaphoreType.DMA((part // rows,)),
        ],
        input_output_aliases={} if done is None else {2 + n: 0},
        cost_estimate=cost(0.5e9, 4 << 20),
        compiler_params=PARAMS,
        name="last",
    )(*in_vmem([base, right]), *data, *extra)


def core_swap(value):
    n = lax.axis_size("tp")
    return lax.ppermute(value, "tp", [(i, i ^ 1) for i in range(n)])


def chip_turn(value, by):
    n = lax.axis_size("tp")
    return lax.ppermute(value, "tp", [(i, (i + 2 * by) % n) for i in range(n)])


def gather_tp(value):
    blocks = [value, core_swap(value)]
    for by in range(1, lax.axis_size("tp") // 2):
        far = chip_turn(value, by)
        blocks += [far, core_swap(far)]
    return blocks


def sources():
    n = lax.axis_size("tp")
    me = lax.axis_index("tp")
    out = [me, me ^ 1]
    for by in range(1, n // 2):
        far = lax.rem(me + (n - 2 * by), n)
        out += [far, far ^ 1]
    return out


def output_weights(out_att, out_ret, slabs):
    peers = [core_swap(w) for w in (out_att, out_ret)]
    att, ret = [], []
    for i, piece in enumerate(slabs):
        by = i // 2 + 1
        moved = chip_turn(piece, by)
        (att if i % 2 == 0 else ret).extend([moved, core_swap(moved)])
    return [out_att, out_ret] + peers + att + ret


def body(
    tokens,
    norm_gain,
    att_query,
    att_key,
    att_value,
    ret_query,
    ret_key,
    ret_value,
    ret_gate,
    att_sink,
    decay_log,
    init_state,
    out_att,
    out_ret,
):
    n_sp = lax.axis_size("sp")
    total = tokens.shape[0]
    seq_len = total * n_sp
    width = att_query.shape[1]
    half = width // 2
    kv_local = att_key.shape[1] // HD
    groups = att_sink.shape[0] // kv_local
    ret_local = decay_log.shape[0]
    cols = tokens.shape[1]

    slabs = slab(out_att, out_ret, cols)
    pieces = split(tokens, CHUNKS)
    near = core_swap(tokens)
    far = {}
    for c in ORDER:
        far[c] = []
        for by in range(1, lax.axis_size("tp") // 2):
            block = chip_turn(pieces[c], by)
            far[c] += [block, core_swap(block)]

    lane = np.arange(ret_local * RK)
    swap = np.zeros((lane.size, lane.size), np.float32)
    swap[lane ^ (RK // 2), lane] = np.where(lane % RK < RK // 2, -1.0, 1.0)
    swap = jnp.asarray(swap, BF16)
    mix = np.zeros((width, width), np.float32)
    for g in range(kv_local):
        for j in range(groups):
            for i in range(HD):
                mix[(g * groups + j) * HD + i, (j * kv_local + g) * HD + i] = 1.0
    mix = jnp.asarray(mix, BF16)

    if half % 128 == 0:
        weights = [att_query, att_key, att_value, ret_query, ret_key, ret_value, ret_gate]
        parts = [(0, 0), (1, 0), (1, half), (2, 0), (2, half), (3, 0), (4, 0)]
    else:
        weights = [
            att_query,
            jnp.concatenate([att_key, att_value], axis=1),
            jnp.concatenate([ret_query, ret_key], axis=1),
            ret_value,
            ret_gate,
        ]
        parts = [(i, 0) for i in range(5)]
    gain = norm_gain[None, :]
    weights = in_vmem(weights)
    crow, ccol, cos, sin = prepare(decay_log, [])
    out_w = output_weights(out_att, out_ret, slabs)
    proj = [None] * len(CHUNKS)
    sums = [None] * len(CHUNKS)
    edges = [None] * len(CHUNKS)
    for c in ORDER:
        first, rows = CHUNKS[c][0] * total // 8, CHUNKS[c][1] * total // 8
        proj[c], sums[c], *edges[c] = project(
            gain, ccol, swap, mix, cos, sin, [tokens, near] + far[c], weights, parts,
            first, rows, ret_local, [edges[-1][0]] if c == 0 else [],
        )

    edge0 = lax.ppermute(edges[0][0], "sp", [(i, i ^ 1) for i in range(n_sp)])
    turn = [(i, (((i + 1) ^ 1) + n_sp - 1) % n_sp) for i in range(n_sp)]
    edge1 = lax.ppermute(edges[0][1], "sp", turn)
    sent = totals(ccol, sums, n_sp)
    got = lax.all_to_all(sent, "sp", 0, 0, tiled=True)
    part = total // HALVES
    att_blocks = []
    for i in range(HALVES):
        attended = attend(att_sink, proj, edge0, edge1, kv_local, groups, seq_len, i * part, part)
        att_blocks.append(gather_tp(attended))
    kept = retain(ccol, crow, got, init_state, proj, ret_local, n_sp)
    ret_blocks = [gather_tp(kept[i]) for i in range(HALVES)]
    att_pieces = [block for pair in zip(*att_blocks) for block in pair]
    ret_pieces = [block for pair in zip(*ret_blocks) for block in pair]
    base, right = most(out_w, att_pieces + ret_pieces[: 2 * HALVES], cols)
    done = None
    for i in range(HALVES):
        done = last(base, right, ret_blocks[i][2:], i * part, done)
    return done


def solution(mesh):
    in_specs = (
        P("sp", "tp"),
        P(),
        P(None, "tp"),
        P(None, "tp"),
        P(None, "tp"),
        P(None, "tp"),
        P(None, "tp"),
        P(None, "tp"),
        P(None, "tp"),
        P("tp"),
        P("tp", "sp"),
        P(None, "tp", None, None),
        P("tp", None),
        P("tp", None),
    )
    out_specs = P("sp", "tp")
    return jax.shard_map(body, mesh=mesh, in_specs=in_specs, out_specs=out_specs, check_vma=False)
```

```python
import functools
import math

import jax
import jax.numpy as jnp
import numpy as np
from jax import lax
from jax.experimental import pallas as pl
from jax.experimental.pallas import tpu as pltpu
from jax.sharding import PartitionSpec as P


HD = 64
RK = 64
RV = 128
WINDOW = 128
NORM_EPS = 1e-06
ROPE_BASE = 10000.0
NEG = -1e30
EXTRA = 16
CHUNKS = ((0, 7), (1, 2, 3), (4, 5, 6))
TABLE = 32
HALVES = 2
F32 = jnp.float32
BF16 = jnp.bfloat16

VMEM = pl.BlockSpec(memory_space=pltpu.VMEM)
SMEM = pl.BlockSpec(memory_space=pltpu.SMEM)
HBM = pl.BlockSpec(memory_space=pltpu.HBM)
PARAMS = pltpu.CompilerParams(vmem_limit_bytes=16 << 20)


def cost(flops, nbytes):
    return pl.CostEstimate(flops=int(flops), bytes_accessed=int(nbytes), transcendentals=0)


def dot(a, b):
    return jnp.dot(a, b, preferred_element_type=F32)


def dot_t(a, b):
    return lax.dot_general(a, b, (((1,), (1,)), ((), ())), preferred_element_type=F32)


def t_dot(a, b):
    return lax.dot_general(a, b, (((0,), (0,)), ((), ())), preferred_element_type=F32)


def in_vmem(values):
    return [pltpu.with_memory_space_constraint(v, pltpu.VMEM) for v in values]


def in_hbm(values):
    return [pltpu.with_memory_space_constraint(v, pltpu.HBM) for v in values]


def runs():
    out = []
    for c, eighths in enumerate(CHUNKS):
        for i, e in enumerate(eighths):
            if out and out[-1][0] == c and out[-1][2] + out[-1][3] == e:
                out[-1][3] += 1
            else:
                out.append([c, i, e, 1])
    return sorted(out, key=lambda run: run[2])


class Copies:
    def __init__(self, sems):
        self.sems = sems
        self.copies = []

    def start(self, src, dst):
        copy = pltpu.make_async_copy(src, dst, self.sems.at[len(self.copies)])
        copy.start()
        self.copies.append(copy)

    def wait(self, first=0, last=None):
        for copy in self.copies[first:last]:
            copy.wait()


def slab_kernel(chips, *refs):
    weights = refs[:2]
    slabs = refs[2:-1]
    copies = Copies(refs[-1])
    tp = lax.axis_index("tp")
    for i, slab in enumerate(slabs):
        target = lax.rem(tp // 2 + 1 + i // 2, chips)
        width = slab.shape[1]
        cols = pl.ds(pl.multiple_of(target * width, width), width)
        copies.start(weights[i % 2].at[:, cols], slab)
    copies.wait()


def slab(att, ret, cols):
    chips = lax.axis_size("tp") // 2
    shape = jax.ShapeDtypeStruct((att.shape[0], 2 * cols), BF16)
    return pl.pallas_call(
        functools.partial(slab_kernel, chips),
        out_shape=(shape,) * (2 * chips - 2),
        in_specs=[HBM, HBM],
        out_specs=(VMEM,) * (2 * chips - 2),
        scratch_shapes=[pltpu.SemaphoreType.DMA((2 * chips - 2,))],
        cost_estimate=cost(0.1e9, 3 << 20),
        compiler_params=PARAMS,
        name="slab",
    )(*in_hbm([att, ret]))


def split_kernel(*refs):
    tokens, sems = refs[0], refs[-1]
    copies = Copies(sems)
    size = tokens.shape[0] // 8
    for c, inner, first, count in runs():
        dst = refs[1 + c].at[pl.ds(inner * size, count * size)]
        copies.start(tokens.at[pl.ds(first * size, count * size)], dst)
    copies.wait()


def split(tokens):
    total, cols = tokens.shape
    return pl.pallas_call(
        split_kernel,
        out_shape=tuple(jax.ShapeDtypeStruct((len(e) * total // 8, cols), BF16) for e in CHUNKS),
        in_specs=[HBM],
        out_specs=(VMEM,) * len(CHUNKS),
        scratch_shapes=[pltpu.SemaphoreType.DMA((len(runs()),))],
        cost_estimate=cost(0.1e9, 3 << 20),
        compiler_params=PARAMS,
        name="split",
    )(*in_hbm([tokens]))


def prepare_kernel(log_ref, *refs):
    row_ref, col_ref, cos_ref, sin_ref = refs[-4:]
    total = log_ref.shape[1]
    heads = log_ref.shape[0]
    sums = jnp.concatenate([log_ref[...], jnp.zeros((8 - heads, total), F32)], axis=0)
    lane = lax.broadcasted_iota(jnp.int32, sums.shape, 1)
    step = 1
    while step < total:
        sums = sums + jnp.where(lane >= step, pltpu.roll(sums, step, 1), 0.0)
        step *= 2
    row_ref[...] = sums
    col_ref[...] = sums.T
    rows, lanes = cos_ref.shape
    row = lax.broadcasted_iota(jnp.int32, (rows, lanes), 0)
    pair = lax.broadcasted_iota(jnp.int32, (rows, lanes), 1) & (RK // 2 - 1)
    count = total // TABLE
    place = jnp.where(row < count, lax.axis_index("sp") * total + TABLE * row, row - count)
    inverse = jnp.exp(pair.astype(F32) * (-2.0 * math.log(ROPE_BASE) / RK))
    angles = place.astype(F32) * inverse
    cos_ref[...] = jnp.cos(angles)
    sin_ref[...] = jnp.sin(angles)


def prepare(log, weights):
    heads, total = log.shape
    table = jax.ShapeDtypeStruct((total // TABLE + TABLE, heads * RK), F32)
    return pl.pallas_call(
        prepare_kernel,
        out_shape=(
            jax.ShapeDtypeStruct((8, total), F32),
            jax.ShapeDtypeStruct((total, 8), F32),
            table,
            table,
        ),
        in_specs=[VMEM] * (1 + len(weights)),
        out_specs=(VMEM,) * 4,
        cost_estimate=cost(8e9, 1 << 16),
        compiler_params=PARAMS,
        name="prepare",
    )(log, *weights)


def project_kernel(n_blocks, n_w, parts, eighths, ret_local, *refs):
    gain_ref, ccol_ref, swap_ref, mix_ref, cos_ref, sin_ref = refs[:6]
    blocks = refs[6 : 6 + n_blocks]
    w_refs = refs[6 + n_blocks : 6 + n_blocks + n_w]
    out_ref, sum_ref = refs[6 + n_blocks + n_w : 8 + n_blocks + n_w]
    edge_refs = refs[8 + n_blocks + n_w : -4]
    xn, inv, held, sems = refs[-4:]
    copies = Copies(sems)
    width = blocks[0].shape[1]
    rows = xn.shape[0]
    group_width = inv.shape[1]
    half = group_width // 2
    total = ccol_ref.shape[0]
    starts = [pl.multiple_of(i * width, width) for i in sources()]
    tile = total // 8
    lanes = min(128, width)
    for r, eighth in enumerate(eighths):
        here = pl.ds(r * tile, tile)
        squares = jnp.zeros((tile, lanes), F32)
        for start, block in zip(starts, blocks):
            at = here if block.shape[0] == rows else pl.ds(eighth * tile, tile)
            for low in range(0, width, lanes):
                part = block[at, low : low + lanes].astype(F32)
                squares = squares + part * part
                col = pl.ds(pl.multiple_of(start + low, lanes), lanes)
                xn[here, col] = (part * gain_ref[:, col]).astype(BF16)
        mean = jnp.sum(squares, axis=1, keepdims=True) / (width * n_blocks)
        inv[here, :] = jnp.broadcast_to(lax.rsqrt(mean + NORM_EPS), (tile, group_width))
    count = total // TABLE
    cos_b, sin_b = cos_ref[count:], sin_ref[count:]
    cosines, sines = [], []
    for k in [e * tile // TABLE + i for e in eighths for i in range(tile // TABLE)]:
        cos_k, sin_k = cos_ref[k : k + 1], sin_ref[k : k + 1]
        cosines.append(cos_k * cos_b - sin_k * sin_b)
        sines.append(sin_k * cos_b + cos_k * sin_b)
    cosine = jnp.concatenate(cosines, axis=0)
    sine = jnp.concatenate(sines, axis=0)
    for group in (2, 3, 0, 1, 4):
        ws = [w[...] for w, (g, _) in zip(w_refs, parts) if g == group]
        w = ws[0] if len(ws) == 1 else jnp.concatenate(ws, axis=1)
        raw = (dot(xn[...], w) * inv[...]).astype(BF16)
        if group == 0:
            raw = (dot(raw, mix_ref[...]) * HD ** (-0.5)).astype(BF16)
        if group == 2:
            sides = []
            for low, scale in ((0, 1.0), (half, RK ** (-0.5))):
                side = raw[:, low : low + half]
                turned = side.astype(F32) * cosine + dot(side, swap_ref[...]) * sine
                sides.append((turned * scale).astype(BF16))
            keys = sides[1]
            raw = jnp.concatenate(sides, axis=1)
        if group == 3:
            for h in range(ret_local):
                col = [ccol_ref[e * tile : (e + 1) * tile, h : h + 1] for e in eighths]
                col = jnp.concatenate(col, axis=0)
                end = ccol_ref[total - 1 : total, h : h + 1]
                v = raw[:, h * RV : (h + 1) * RV].astype(F32)
                both = jnp.concatenate([v * jnp.exp(end - col), v * jnp.exp(col)], axis=1)
                sum_ref[h] = t_dot(keys, both.astype(BF16))[h * RK : (h + 1) * RK]
        if group == 1 and edge_refs:
            even = lax.rem(lax.axis_index("sp"), 2) == 0
            edge_refs[0][...] = jnp.where(even, raw[rows - WINDOW :], raw[:WINDOW])
            edge_refs[1][...] = jnp.where(even, raw[:WINDOW], raw[rows - WINDOW :])
        held[group] = raw
        copies.start(held.at[group], out_ref.at[group])
    copies.wait()


def project(gain, ccol, swap, mix, cos, sin, blocks, weights, parts, eighths, ret_local):
    width = mix.shape[0]
    depth = gain.shape[1]
    n = len(blocks)
    rows = len(eighths) * ccol.shape[0] // 8
    n_edges = 2 if eighths[0] == 0 and eighths[-1] == 7 else 0
    return pl.pallas_call(
        functools.partial(project_kernel, n, len(weights), parts, eighths, ret_local),
        out_shape=(
            pltpu.HBM((5, rows, width), BF16),
            pltpu.VMEM((ret_local, RK, 2 * RV), F32),
            *[jax.ShapeDtypeStruct((WINDOW, width), BF16)] * n_edges,
        ),
        in_specs=[VMEM] * (n + 6 + len(weights)),
        out_specs=(HBM, VMEM) + (VMEM,) * n_edges,
        scratch_shapes=[
            pltpu.VMEM((rows, depth), BF16),
            pltpu.VMEM((rows, width), F32),
            pltpu.VMEM((5, rows, width), BF16),
            pltpu.SemaphoreType.DMA((5,)),
        ],
        cost_estimate=cost(2 * rows * depth * 5 * width // 4, 7 << 20),
        compiler_params=PARAMS,
        name="project",
    )(gain, ccol, swap, mix, cos, sin, *blocks, *weights)


def overlaps(sizes, first, rows):
    out = []
    at = 0
    for i, size in enumerate(sizes):
        low, high = max(at, first), min(at + size, first + rows)
        if low < high:
            out.append((i, low - at, high - low, low - first))
        at += size
    return out


def attend_kernel(n_chunks, kv_local, groups, seq_len, total, start, *refs):
    sink_ref = refs[0]
    proj = refs[1 : 1 + n_chunks]
    low_ref, high_ref, out_ref = refs[1 + n_chunks : 4 + n_chunks]
    qbuf, kvbuf, vbuf, mask, sems = refs[-5:]
    copies = Copies(sems)
    rows = out_ref.shape[0]
    offset = lax.axis_index("sp") * total
    kv_cols = kv_local * HD
    block = WINDOW
    span = block + 2 * WINDOW
    size = total // 8
    order = runs()
    sizes = [WINDOW] + [run[3] * size for run in order] + [WINDOW]
    for i, low, count, to in overlaps(sizes, start, rows + 2 * WINDOW):
        if i in (0, len(order) + 1):
            even = lax.rem(lax.axis_index("sp"), 2) == 0
            here = pl.ds(low, count)
            near, far = (high_ref, low_ref) if i == 0 else (low_ref, high_ref)
            kvbuf[pl.ds(to, count)] = jnp.where(even, near[here], far[here])
        else:
            c, inner = order[i - 1][:2]
            src = proj[c].at[1, pl.ds(inner * size + low, count)]
            copies.start(src, kvbuf.at[pl.ds(to, count)])
    n_kv = len(copies.copies)
    for i, low, count, to in overlaps(sizes[1:-1], start, rows):
        c, inner = order[i][:2]
        src = proj[c].at[0, pl.ds(inner * size + low, count)]
        copies.start(src, qbuf.at[pl.ds(to, count)])
    vbuf[kv_cols:] = jnp.ones((vbuf.shape[0] - kv_cols, vbuf.shape[1]), BF16)
    row = lax.broadcasted_iota(jnp.int32, (span, block), 1)
    col = lax.broadcasted_iota(jnp.int32, (span, block), 0)
    band = (col >= row) & (col <= row + 2 * WINDOW)
    n_steps = rows // block
    edges = [i for i in range(n_steps) if start + i * block in (0, total - block)]
    inner = jnp.where(band, 0.0, NEG)
    mask[0] = jnp.concatenate([inner] * groups, axis=1)
    for kind, i in enumerate(edges, 1):
        pos = col + (offset + start + i * block - WINDOW)
        one = jnp.where((pos >= 0) & (pos < seq_len), inner, NEG)
        mask[kind] = jnp.concatenate([one] * groups, axis=1)
    copies.wait(0, n_kv)
    for i in range(kvbuf.shape[0] // block):
        here = pl.ds(i * block, block)
        vbuf[0:kv_cols, here] = kvbuf[here, kv_cols:].T
    copies.wait(n_kv)
    lane = lax.broadcasted_iota(jnp.int32, (block, kv_cols), 1)
    for i in range(n_steps):
        first = i * block
        q = qbuf[pl.ds(first, block)]
        k = kvbuf[pl.ds(first, span), :kv_cols]
        bias = mask[edges.index(i) + 1 if i in edges else 0]
        scores = []
        for g in range(kv_local):
            mine = (lane >= g * HD) & (lane < (g + 1) * HD)
            tiles = []
            for j in range(groups):
                tile = q[:, j * kv_cols : (j + 1) * kv_cols]
                tiles.append(jnp.where(mine, tile, jnp.zeros_like(tile)))
            scores.append(dot_t(k, jnp.concatenate(tiles, axis=0)))
        weights = []
        rests = []
        for g in range(kv_local):
            s = scores[g] + bias
            sink = jnp.concatenate(
                [jnp.full((1, block), sink_ref[g * groups + j], F32) for j in range(groups)], axis=1
            )
            top = jnp.maximum(jnp.max(s, axis=0, keepdims=True), sink)
            weights.append(jnp.exp(s - top).astype(BF16))
            rests.append(jnp.exp(sink - top))
        outs = []
        for g in range(kv_local):
            v = vbuf[g * HD : (g + 1) * HD, pl.ds(first, span)]
            ones = vbuf[kv_cols : kv_cols + 16, pl.ds(first, span)]
            o = dot(jnp.concatenate([v, ones], axis=0), weights[g])
            o = o[:HD] / (o[HD : HD + 1] + rests[g])
            outs += [o[:, j * block : (j + 1) * block] for j in range(groups)]
        out_ref[pl.ds(first, block)] = jnp.concatenate(outs, axis=0).T.astype(BF16)


def attend(sink, proj, low, high, kv_local, groups, seq_len, start, rows):
    n = len(proj)
    width = proj[0].shape[2]
    total = sum(p.shape[1] for p in proj)
    kv_cols = kv_local * HD
    return pl.pallas_call(
        functools.partial(attend_kernel, n, kv_local, groups, seq_len, total, start),
        out_shape=jax.ShapeDtypeStruct((rows, width), BF16),
        in_specs=[SMEM] + [HBM] * n + [VMEM, VMEM],
        out_specs=VMEM,
        scratch_shapes=[
            pltpu.VMEM((rows, width), BF16),
            pltpu.VMEM((rows + 2 * WINDOW, 2 * kv_cols), BF16),
            pltpu.VMEM((kv_cols + 16, rows + 2 * WINDOW), BF16),
            pltpu.VMEM((3, 3 * WINDOW, groups * WINDOW), F32),
            pltpu.SemaphoreType.DMA((2 * len(runs()),)),
        ],
        cost_estimate=cost(0.8e9, 3 << 20),
        compiler_params=PARAMS,
        name="attend",
    )(sink, *in_hbm(proj), low, high)


def totals_kernel(n_chunks, ret_local, n_sp, *refs):
    ccol_ref = refs[0]
    sum_refs = refs[1 : 1 + n_chunks]
    out_ref = refs[-1]
    me = lax.axis_index("sp")
    last = ccol_ref.shape[0] - 1
    line = lax.broadcasted_iota(jnp.int32, (EXTRA, RV), 0)
    for h in range(ret_local):
        sums = sum_refs[0][h]
        for ref in sum_refs[1:]:
            sums = sums + ref[h]
        end = jnp.broadcast_to(ccol_ref[last : last + 1, h : h + 1], (EXTRA, RV))
        d0 = end.astype(BF16).astype(F32)
        d1 = (end - d0).astype(BF16).astype(F32)
        d2 = end - d0 - d1
        extra = jnp.where(line == 0, d0, jnp.where(line == 1, d1, jnp.where(line == 2, d2, 0.0)))
        fwd = jnp.concatenate([sums[:, :RV], extra], axis=0).astype(BF16)
        bwd = jnp.concatenate([sums[:, RV:], extra], axis=0).astype(BF16)
        for j in range(n_sp):
            out_ref[j, h] = jnp.where(j > me, fwd, bwd)


def totals(ccol, sums, n_sp):
    ret_local = sums[0].shape[0]
    return pl.pallas_call(
        functools.partial(totals_kernel, len(sums), ret_local, n_sp),
        out_shape=jax.ShapeDtypeStruct((n_sp, ret_local, RK + EXTRA, RV), BF16),
        in_specs=[VMEM] * (1 + len(sums)),
        out_specs=VMEM,
        cost_estimate=cost(0.1e9, 1 << 20),
        compiler_params=PARAMS,
        name="totals",
    )(ccol, *sums)


def retain_kernel(n_chunks, ret_local, n_sp, *refs):
    ccol_hbm, crow_hbm, got_hbm, init_hbm = refs[:4]
    proj = refs[4 : 4 + n_chunks]
    outs = refs[4 + n_chunks : 4 + n_chunks + HALVES]
    states, got_ref, init_ref, ccol_ref, crow_ref, rbuf, vbuf, gbuf, sems = refs[-9:]
    me = lax.axis_index("sp")
    total = ccol_ref.shape[0]
    last = total - 1
    cols = ret_local * RK
    copies = Copies(sems)
    copies.start(got_hbm, got_ref)
    copies.start(init_hbm, init_ref)
    copies.start(ccol_hbm, ccol_ref)
    copies.start(crow_hbm, crow_ref)
    size = total // 8
    for group, buf in ((2, rbuf), (3, vbuf), (4, gbuf)):
        for c, inner, first, count in runs():
            src = proj[c].at[group, pl.ds(inner * size, count * size)]
            copies.start(src, buf.at[pl.ds(first * size, count * size)])
    copies.wait(0, 2)
    states[...] = jnp.zeros(states.shape, BF16)
    for h in range(ret_local):
        ends = []
        for j in range(n_sp):
            tail = got_ref[j, h, RK : RK + EXTRA, :].astype(F32)
            ends.append(jnp.sum(tail, axis=0, keepdims=True))
        for side, order in enumerate((range(n_sp - 1, -1, -1), range(n_sp))):
            state = jnp.zeros((RK, RV), F32)
            run = jnp.zeros((1, RV), F32)
            for j in order:
                here = (j < me) if side == 0 else (j > me)
                term = jnp.exp(run) * got_ref[j, h, 0:RK, :].astype(F32)
                state = state + jnp.where(here, term, 0.0)
                run = run + jnp.where(here, ends[j], 0.0)
            state = state + jnp.exp(run) * init_ref[side, h]
            col = (2 * h + side) * RV
            states[h * RK : (h + 1) * RK, col : col + RV] = state.astype(BF16)
    copies.wait(2)
    block = min(256, total // HALVES)
    lane = lax.broadcasted_iota(jnp.int32, (block, cols), 1)
    for i in range(total // block):
        here = pl.ds(i * block, block)
        out_ref = outs[i * block * HALVES // total]
        there = pl.ds(i * block % (total // HALVES), block)
        q = rbuf[here, :cols]
        both = dot(q, states[...])
        for h in range(ret_local):
            mine = (lane >= h * RK) & (lane < (h + 1) * RK)
            qh = jnp.where(mine, q, jnp.zeros_like(q))
            col = ccol_ref[here, h : h + 1]
            end = ccol_ref[last : last + 1, h : h + 1]
            gap = col - crow_ref[h : h + 1, :]
            w = (dot_t(qh, rbuf[:, cols:]) * jnp.exp(-jnp.abs(gap))).astype(BF16)
            ret = (
                dot(w, vbuf[:, h * RV : (h + 1) * RV])
                + jnp.exp(col) * both[:, 2 * h * RV : (2 * h + 1) * RV]
                + jnp.exp(end - col) * both[:, (2 * h + 1) * RV : (2 * h + 2) * RV]
            )
            centered = ret - jnp.mean(ret, axis=1, keepdims=True)
            scale = lax.rsqrt(jnp.mean(centered * centered, axis=1, keepdims=True) + NORM_EPS)
            gate = gbuf[here, h * RV : (h + 1) * RV].astype(F32)
            gated = gate / (1.0 + jnp.exp(-gate))
            out_ref[there, h * RV : (h + 1) * RV] = (gated * (centered * scale)).astype(BF16)


def retain(ccol, crow, got, init, proj, ret_local, n_sp):
    n = len(proj)
    width = proj[0].shape[2]
    total = ccol.shape[0]
    return pl.pallas_call(
        functools.partial(retain_kernel, n, ret_local, n_sp),
        out_shape=(jax.ShapeDtypeStruct((total // HALVES, width), BF16),) * HALVES,
        in_specs=[HBM] * (n + 4),
        out_specs=(VMEM,) * HALVES,
        scratch_shapes=[
            pltpu.VMEM((ret_local * RK, 2 * ret_local * RV), BF16),
            pltpu.VMEM(got.shape, BF16),
            pltpu.VMEM(init.shape, F32),
            pltpu.VMEM(ccol.shape, F32),
            pltpu.VMEM(crow.shape, F32),
            pltpu.VMEM((total, width), BF16),
            pltpu.VMEM((total, width), BF16),
            pltpu.VMEM((total, width), BF16),
            pltpu.SemaphoreType.DMA((3 * len(runs()) + 4,)),
        ],
        cost_estimate=cost(1.5e9, 4 << 20),
        compiler_params=PARAMS,
        name="retain",
    )(*in_hbm([ccol, crow, got, init, *proj]))


def most_kernel(n_far, n_data, *refs):
    near_att, near_ret, peer_att, peer_ret = refs[:4]
    far_att, far_ret = refs[4 : 4 + n_far], refs[4 + n_far : 4 + 2 * n_far]
    data = refs[4 + 2 * n_far : 4 + 2 * n_far + n_data]
    out_ref, rest_ref = refs[4 + 2 * n_far + n_data : 6 + 2 * n_far + n_data]
    left, right, sems = refs[-3:]
    copies = Copies(sems)
    cols = out_ref.shape[1]
    tp = lax.axis_index("tp")
    mine = pl.ds(pl.multiple_of(tp * cols, cols), cols)
    half = pl.ds(pl.multiple_of(lax.rem(tp, 2) * cols, cols), cols)
    depth = near_att.shape[0]
    rows = [(ref, mine) for ref in (near_att, peer_att)] + [(ref, half) for ref in far_att]
    rows += [(ref, mine) for ref in (near_ret, peer_ret)]
    for i, (ref, at) in enumerate(rows):
        copies.start(ref.at[:, at], right.at[pl.ds(i * depth, depth)])
    for i, ref in enumerate(data):
        half_rows = pl.ds(i % HALVES * ref.shape[0], ref.shape[0])
        copies.start(ref, left.at[half_rows, pl.ds(i // HALVES * depth, depth)])
    for i, ref in enumerate(far_ret):
        copies.start(ref.at[:, half], rest_ref.at[pl.ds(i * depth, depth)])
    copies.wait()
    rows = min(256, out_ref.shape[0])
    for i in range(out_ref.shape[0] // rows):
        here = pl.ds(i * rows, rows)
        out_ref[here] = dot(left[here], right[...])


def most(weights, data, cols):
    total, depth = data[0].shape[0] * HALVES, data[0].shape[1]
    n = len(data)
    n_far = (len(weights) - 4) // 2
    return pl.pallas_call(
        functools.partial(most_kernel, n_far, n),
        out_shape=(
            pltpu.VMEM((total, cols), F32),
            pltpu.VMEM((n_far * depth, cols), BF16),
        ),
        in_specs=[HBM] * (len(weights) + n),
        out_specs=(VMEM, VMEM),
        scratch_shapes=[
            pltpu.VMEM((total, n // HALVES * depth), BF16),
            pltpu.VMEM((n // HALVES * depth, cols), BF16),
            pltpu.SemaphoreType.DMA((len(weights) + n,)),
        ],
        cost_estimate=cost(1e9, 8 << 20),
        compiler_params=PARAMS,
        name="most",
    )(*in_hbm(weights), *in_hbm(data))


def last_kernel(n_data, start, *refs):
    base, right = refs[:2]
    data = refs[2 : 2 + n_data]
    out_ref, held, sems = refs[-3:]
    copies = Copies(sems)
    rows = held.shape[1]
    for i in range(held.shape[0]):
        here = pl.ds(i * rows, rows)
        there = pl.ds(start + i * rows, rows)
        part = dot(jnp.concatenate([ref[here] for ref in data], axis=1), right[...])
        held[i] = (part + base[there]).astype(BF16)
        copies.start(held.at[i], out_ref.at[there])
    copies.wait()


def last(base, right, data, start, done):
    total, cols = base.shape
    part = data[0].shape[0]
    rows = min(256, part)
    n = len(data)
    extra = [] if done is None else [done]
    return pl.pallas_call(
        functools.partial(last_kernel, n, start),
        out_shape=jax.ShapeDtypeStruct((total, cols), BF16),
        in_specs=[VMEM] * (2 + n) + [HBM] * len(extra),
        out_specs=HBM,
        scratch_shapes=[
            pltpu.VMEM((part // rows, rows, cols), BF16),
            pltpu.SemaphoreType.DMA((part // rows,)),
        ],
        input_output_aliases={} if done is None else {2 + n: 0},
        cost_estimate=cost(0.5e9, 4 << 20),
        compiler_params=PARAMS,
        name="last",
    )(*in_vmem([base, right]), *data, *extra)


def core_swap(value):
    n = lax.axis_size("tp")
    return lax.ppermute(value, "tp", [(i, i ^ 1) for i in range(n)])


def chip_turn(value, by):
    n = lax.axis_size("tp")
    return lax.ppermute(value, "tp", [(i, (i + 2 * by) % n) for i in range(n)])


def gather_tp(value):
    blocks = [value, core_swap(value)]
    for by in range(1, lax.axis_size("tp") // 2):
        far = chip_turn(value, by)
        blocks += [far, core_swap(far)]
    return blocks


def sources():
    n = lax.axis_size("tp")
    me = lax.axis_index("tp")
    out = [me, me ^ 1]
    for by in range(1, n // 2):
        far = lax.rem(me + (n - 2 * by), n)
        out += [far, far ^ 1]
    return out


def output_weights(out_att, out_ret, slabs):
    peers = [core_swap(w) for w in (out_att, out_ret)]
    att, ret = [], []
    for i, piece in enumerate(slabs):
        by = i // 2 + 1
        moved = chip_turn(piece, by)
        (att if i % 2 == 0 else ret).extend([moved, core_swap(moved)])
    return [out_att, out_ret] + peers + att + ret


def body(
    tokens,
    norm_gain,
    att_query,
    att_key,
    att_value,
    ret_query,
    ret_key,
    ret_value,
    ret_gate,
    att_sink,
    decay_log,
    init_state,
    out_att,
    out_ret,
):
    n_sp = lax.axis_size("sp")
    total = tokens.shape[0]
    seq_len = total * n_sp
    width = att_query.shape[1]
    half = width // 2
    kv_local = att_key.shape[1] // HD
    groups = att_sink.shape[0] // kv_local
    ret_local = decay_log.shape[0]
    cols = tokens.shape[1]

    slabs = slab(out_att, out_ret, cols)
    pieces = split(tokens)
    near = core_swap(tokens)
    far = {}
    for c in range(len(CHUNKS)):
        far[c] = []
        for by in range(1, lax.axis_size("tp") // 2):
            block = chip_turn(pieces[c], by)
            far[c] += [block, core_swap(block)]

    lane = np.arange(ret_local * RK)
    swap = np.zeros((lane.size, lane.size), np.float32)
    swap[lane ^ (RK // 2), lane] = np.where(lane % RK < RK // 2, -1.0, 1.0)
    swap = jnp.asarray(swap, BF16)
    mix = np.zeros((width, width), np.float32)
    for g in range(kv_local):
        for j in range(groups):
            for i in range(HD):
                mix[(g * groups + j) * HD + i, (j * kv_local + g) * HD + i] = 1.0
    mix = jnp.asarray(mix, BF16)

    if half % 128 == 0:
        weights = [att_query, att_key, att_value, ret_query, ret_key, ret_value, ret_gate]
        parts = [(0, 0), (1, 0), (1, half), (2, 0), (2, half), (3, 0), (4, 0)]
    else:
        weights = [
            att_query,
            jnp.concatenate([att_key, att_value], axis=1),
            jnp.concatenate([ret_query, ret_key], axis=1),
            ret_value,
            ret_gate,
        ]
        parts = [(i, 0) for i in range(5)]
    gain = norm_gain[None, :]
    weights = in_vmem(weights)
    crow, ccol, cos, sin = prepare(decay_log, [])
    out_w = output_weights(out_att, out_ret, slabs)
    proj = [None] * len(CHUNKS)
    sums = [None] * len(CHUNKS)
    edges = []
    for c, eighths in enumerate(CHUNKS):
        proj[c], sums[c], *found = project(
            gain, ccol, swap, mix, cos, sin, [tokens, near] + far[c], weights, parts,
            eighths, ret_local,
        )
        edges += found

    edge0 = lax.ppermute(edges[0], "sp", [(i, i ^ 1) for i in range(n_sp)])
    turn = [(i, (((i + 1) ^ 1) + n_sp - 1) % n_sp) for i in range(n_sp)]
    edge1 = lax.ppermute(edges[1], "sp", turn)
    sent = totals(ccol, sums, n_sp)
    got = lax.all_to_all(sent, "sp", 0, 0, tiled=True)
    part = total // HALVES
    att_blocks = []
    for i in range(HALVES):
        attended = attend(att_sink, proj, edge0, edge1, kv_local, groups, seq_len, i * part, part)
        att_blocks.append(gather_tp(attended))
    kept = retain(ccol, crow, got, init_state, proj, ret_local, n_sp)
    ret_blocks = [gather_tp(kept[i]) for i in range(HALVES)]
    att_pieces = [block for pair in zip(*att_blocks) for block in pair]
    ret_pieces = [block for pair in zip(*ret_blocks) for block in pair]
    base, right = most(out_w, att_pieces + ret_pieces[: 2 * HALVES], cols)
    done = None
    for i in range(HALVES):
        done = last(base, right, ret_blocks[i][2:], i * part, done)
    return done


def solution(mesh):
    in_specs = (
        P("sp", "tp"),
        P(),
        P(None, "tp"),
        P(None, "tp"),
        P(None, "tp"),
        P(None, "tp"),
        P(None, "tp"),
        P(None, "tp"),
        P(None, "tp"),
        P("tp"),
        P("tp", "sp"),
        P(None, "tp", None, None),
        P("tp", None),
        P("tp", None),
    )
    out_specs = P("sp", "tp")
    return jax.shard_map(body, mesh=mesh, in_specs=in_specs, out_specs=out_specs, check_vma=False)
```

```python
import functools
import math

import jax
import jax.numpy as jnp
import numpy as np
from jax import lax
from jax.experimental import pallas as pl
from jax.experimental.pallas import tpu as pltpu
from jax.sharding import PartitionSpec as P


HD = 64
RK = 64
RV = 128
WINDOW = 128
NORM_EPS = 1e-06
ROPE_BASE = 10000.0
NEG = -1e30
EXTRA = 16
CHUNKS = ((0, 7), (1, 2, 3), (4, 5, 6))
TABLE = 32
HALVES = 2
F32 = jnp.float32
BF16 = jnp.bfloat16

VMEM = pl.BlockSpec(memory_space=pltpu.VMEM)
SMEM = pl.BlockSpec(memory_space=pltpu.SMEM)
HBM = pl.BlockSpec(memory_space=pltpu.HBM)
PARAMS = pltpu.CompilerParams(vmem_limit_bytes=16 << 20)


def cost(flops, nbytes):
    return pl.CostEstimate(flops=int(flops), bytes_accessed=int(nbytes), transcendentals=0)


def dot(a, b):
    return jnp.dot(a, b, preferred_element_type=F32)


def dot_t(a, b):
    return lax.dot_general(a, b, (((1,), (1,)), ((), ())), preferred_element_type=F32)


def t_dot(a, b):
    return lax.dot_general(a, b, (((0,), (0,)), ((), ())), preferred_element_type=F32)


def in_vmem(values):
    return [pltpu.with_memory_space_constraint(v, pltpu.VMEM) for v in values]


def in_hbm(values):
    return [pltpu.with_memory_space_constraint(v, pltpu.HBM) for v in values]


def runs():
    out = []
    for c, eighths in enumerate(CHUNKS):
        for i, e in enumerate(eighths):
            if out and out[-1][0] == c and out[-1][2] + out[-1][3] == e:
                out[-1][3] += 1
            else:
                out.append([c, i, e, 1])
    return sorted(out, key=lambda run: run[2])


class Copies:
    def __init__(self, sems):
        self.sems = sems
        self.copies = []

    def start(self, src, dst):
        copy = pltpu.make_async_copy(src, dst, self.sems.at[len(self.copies)])
        copy.start()
        self.copies.append(copy)

    def wait(self, first=0, last=None):
        for copy in self.copies[first:last]:
            copy.wait()


def slab_kernel(chips, *refs):
    weights = refs[:2]
    slabs = refs[2:-1]
    copies = Copies(refs[-1])
    tp = lax.axis_index("tp")
    for i, slab in enumerate(slabs):
        target = lax.rem(tp // 2 + 1 + i // 2, chips)
        width = slab.shape[1]
        cols = pl.ds(pl.multiple_of(target * width, width), width)
        copies.start(weights[i % 2].at[:, cols], slab)
    copies.wait()


def slab(att, ret, cols):
    chips = lax.axis_size("tp") // 2
    shape = jax.ShapeDtypeStruct((att.shape[0], 2 * cols), BF16)
    return pl.pallas_call(
        functools.partial(slab_kernel, chips),
        out_shape=(shape,) * (2 * chips - 2),
        in_specs=[HBM, HBM],
        out_specs=(VMEM,) * (2 * chips - 2),
        scratch_shapes=[pltpu.SemaphoreType.DMA((2 * chips - 2,))],
        cost_estimate=cost(0.1e9, 3 << 20),
        compiler_params=PARAMS,
        name="slab",
    )(*in_hbm([att, ret]))


def split_kernel(low, high, *refs):
    tokens, sems = refs[0], refs[-1]
    copies = Copies(sems)
    size = tokens.shape[0] // 8
    for c, inner, first, count in runs():
        if not low <= c < high:
            continue
        dst = refs[1 + c - low].at[pl.ds(inner * size, count * size)]
        copies.start(tokens.at[pl.ds(first * size, count * size)], dst)
    copies.wait()


def split(tokens, low, high):
    total, cols = tokens.shape
    sizes = [len(e) * total // 8 for e in CHUNKS[low:high]]
    return pl.pallas_call(
        functools.partial(split_kernel, low, high),
        out_shape=tuple(jax.ShapeDtypeStruct((size, cols), BF16) for size in sizes),
        in_specs=[HBM],
        out_specs=(VMEM,) * len(sizes),
        scratch_shapes=[pltpu.SemaphoreType.DMA((len(runs()),))],
        cost_estimate=cost(0.1e9, 3 << 20),
        compiler_params=PARAMS,
        name="split",
    )(*in_hbm([tokens]))


def prepare_kernel(log_ref, *refs):
    row_ref, col_ref, cos_ref, sin_ref = refs[-4:]
    total = log_ref.shape[1]
    heads = log_ref.shape[0]
    sums = jnp.concatenate([log_ref[...], jnp.zeros((8 - heads, total), F32)], axis=0)
    lane = lax.broadcasted_iota(jnp.int32, sums.shape, 1)
    step = 1
    while step < total:
        sums = sums + jnp.where(lane >= step, pltpu.roll(sums, step, 1), 0.0)
        step *= 2
    row_ref[...] = sums
    col_ref[...] = sums.T
    rows, lanes = cos_ref.shape
    row = lax.broadcasted_iota(jnp.int32, (rows, lanes), 0)
    pair = lax.broadcasted_iota(jnp.int32, (rows, lanes), 1) & (RK // 2 - 1)
    count = total // TABLE
    place = jnp.where(row < count, lax.axis_index("sp") * total + TABLE * row, row - count)
    inverse = jnp.exp(pair.astype(F32) * (-2.0 * math.log(ROPE_BASE) / RK))
    angles = place.astype(F32) * inverse
    cos_ref[...] = jnp.cos(angles)
    sin_ref[...] = jnp.sin(angles)


def prepare(log, weights):
    heads, total = log.shape
    table = jax.ShapeDtypeStruct((total // TABLE + TABLE, heads * RK), F32)
    return pl.pallas_call(
        prepare_kernel,
        out_shape=(
            jax.ShapeDtypeStruct((8, total), F32),
            jax.ShapeDtypeStruct((total, 8), F32),
            table,
            table,
        ),
        in_specs=[VMEM] * (1 + len(weights)),
        out_specs=(VMEM,) * 4,
        cost_estimate=cost(8e9, 1 << 16),
        compiler_params=PARAMS,
        name="prepare",
    )(log, *weights)


def project_kernel(n_blocks, n_w, parts, eighths, ret_local, *refs):
    gain_ref, ccol_ref, swap_ref, mix_ref, cos_ref, sin_ref = refs[:6]
    blocks = refs[6 : 6 + n_blocks]
    w_refs = refs[6 + n_blocks : 6 + n_blocks + n_w]
    out_ref, sum_ref = refs[6 + n_blocks + n_w : 8 + n_blocks + n_w]
    edge_refs = refs[8 + n_blocks + n_w : -4]
    xn, inv, held, sems = refs[-4:]
    copies = Copies(sems)
    width = blocks[0].shape[1]
    rows = xn.shape[0]
    group_width = inv.shape[1]
    half = group_width // 2
    total = ccol_ref.shape[0]
    starts = [pl.multiple_of(i * width, width) for i in sources()]
    tile = total // 8
    lanes = min(128, width)
    for r, eighth in enumerate(eighths):
        here = pl.ds(r * tile, tile)
        squares = jnp.zeros((tile, lanes), F32)
        for start, block in zip(starts, blocks):
            at = here if block.shape[0] == rows else pl.ds(eighth * tile, tile)
            for low in range(0, width, lanes):
                part = block[at, low : low + lanes].astype(F32)
                squares = squares + part * part
                col = pl.ds(pl.multiple_of(start + low, lanes), lanes)
                xn[here, col] = (part * gain_ref[:, col]).astype(BF16)
        mean = jnp.sum(squares, axis=1, keepdims=True) / (width * n_blocks)
        inv[here, :] = jnp.broadcast_to(lax.rsqrt(mean + NORM_EPS), (tile, group_width))
    count = total // TABLE
    cos_b, sin_b = cos_ref[count:], sin_ref[count:]
    cosines, sines = [], []
    for k in [e * tile // TABLE + i for e in eighths for i in range(tile // TABLE)]:
        cos_k, sin_k = cos_ref[k : k + 1], sin_ref[k : k + 1]
        cosines.append(cos_k * cos_b - sin_k * sin_b)
        sines.append(sin_k * cos_b + cos_k * sin_b)
    cosine = jnp.concatenate(cosines, axis=0)
    sine = jnp.concatenate(sines, axis=0)
    for group in (2, 3, 0, 1, 4):
        ws = [w[...] for w, (g, _) in zip(w_refs, parts) if g == group]
        w = ws[0] if len(ws) == 1 else jnp.concatenate(ws, axis=1)
        raw = (dot(xn[...], w) * inv[...]).astype(BF16)
        if group == 0:
            raw = (dot(raw, mix_ref[...]) * HD ** (-0.5)).astype(BF16)
        if group == 2:
            sides = []
            for low, scale in ((0, 1.0), (half, RK ** (-0.5))):
                side = raw[:, low : low + half]
                turned = side.astype(F32) * cosine + dot(side, swap_ref[...]) * sine
                sides.append((turned * scale).astype(BF16))
            keys = sides[1]
            raw = jnp.concatenate(sides, axis=1)
        if group == 3:
            for h in range(ret_local):
                col = [ccol_ref[e * tile : (e + 1) * tile, h : h + 1] for e in eighths]
                col = jnp.concatenate(col, axis=0)
                end = ccol_ref[total - 1 : total, h : h + 1]
                v = raw[:, h * RV : (h + 1) * RV].astype(F32)
                both = jnp.concatenate([v * jnp.exp(end - col), v * jnp.exp(col)], axis=1)
                sum_ref[h] = t_dot(keys, both.astype(BF16))[h * RK : (h + 1) * RK]
        if group == 1 and edge_refs:
            even = lax.rem(lax.axis_index("sp"), 2) == 0
            edge_refs[0][...] = jnp.where(even, raw[rows - WINDOW :], raw[:WINDOW])
            edge_refs[1][...] = jnp.where(even, raw[:WINDOW], raw[rows - WINDOW :])
        held[group] = raw
        copies.start(held.at[group], out_ref.at[group])
    copies.wait()


def project(gain, ccol, swap, mix, cos, sin, blocks, weights, parts, eighths, ret_local):
    width = mix.shape[0]
    depth = gain.shape[1]
    n = len(blocks)
    rows = len(eighths) * ccol.shape[0] // 8
    n_edges = 2 if eighths[0] == 0 and eighths[-1] == 7 else 0
    return pl.pallas_call(
        functools.partial(project_kernel, n, len(weights), parts, eighths, ret_local),
        out_shape=(
            pltpu.HBM((5, rows, width), BF16),
            pltpu.VMEM((ret_local, RK, 2 * RV), F32),
            *[jax.ShapeDtypeStruct((WINDOW, width), BF16)] * n_edges,
        ),
        in_specs=[VMEM] * (n + 6 + len(weights)),
        out_specs=(HBM, VMEM) + (VMEM,) * n_edges,
        scratch_shapes=[
            pltpu.VMEM((rows, depth), BF16),
            pltpu.VMEM((rows, width), F32),
            pltpu.VMEM((5, rows, width), BF16),
            pltpu.SemaphoreType.DMA((5,)),
        ],
        cost_estimate=cost(2 * rows * depth * 5 * width // 4, 7 << 20),
        compiler_params=PARAMS,
        name="project",
    )(gain, ccol, swap, mix, cos, sin, *blocks, *weights)


def overlaps(sizes, first, rows):
    out = []
    at = 0
    for i, size in enumerate(sizes):
        low, high = max(at, first), min(at + size, first + rows)
        if low < high:
            out.append((i, low - at, high - low, low - first))
        at += size
    return out


def attend_kernel(n_chunks, kv_local, groups, seq_len, total, start, *refs):
    sink_ref = refs[0]
    proj = refs[1 : 1 + n_chunks]
    low_ref, high_ref, out_ref = refs[1 + n_chunks : 4 + n_chunks]
    qbuf, kvbuf, vbuf, mask, sems = refs[-5:]
    copies = Copies(sems)
    rows = out_ref.shape[0]
    offset = lax.axis_index("sp") * total
    kv_cols = kv_local * HD
    block = WINDOW
    span = block + 2 * WINDOW
    size = total // 8
    order = runs()
    sizes = [WINDOW] + [run[3] * size for run in order] + [WINDOW]
    for i, low, count, to in overlaps(sizes, start, rows + 2 * WINDOW):
        if i in (0, len(order) + 1):
            even = lax.rem(lax.axis_index("sp"), 2) == 0
            here = pl.ds(low, count)
            near, far = (high_ref, low_ref) if i == 0 else (low_ref, high_ref)
            kvbuf[pl.ds(to, count)] = jnp.where(even, near[here], far[here])
        else:
            c, inner = order[i - 1][:2]
            src = proj[c].at[1, pl.ds(inner * size + low, count)]
            copies.start(src, kvbuf.at[pl.ds(to, count)])
    n_kv = len(copies.copies)
    for i, low, count, to in overlaps(sizes[1:-1], start, rows):
        c, inner = order[i][:2]
        src = proj[c].at[0, pl.ds(inner * size + low, count)]
        copies.start(src, qbuf.at[pl.ds(to, count)])
    vbuf[kv_cols:] = jnp.ones((vbuf.shape[0] - kv_cols, vbuf.shape[1]), BF16)
    row = lax.broadcasted_iota(jnp.int32, (span, block), 1)
    col = lax.broadcasted_iota(jnp.int32, (span, block), 0)
    band = (col >= row) & (col <= row + 2 * WINDOW)
    n_steps = rows // block
    edges = [i for i in range(n_steps) if start + i * block in (0, total - block)]
    inner = jnp.where(band, 0.0, NEG)
    mask[0] = jnp.concatenate([inner] * groups, axis=1)
    for kind, i in enumerate(edges, 1):
        pos = col + (offset + start + i * block - WINDOW)
        one = jnp.where((pos >= 0) & (pos < seq_len), inner, NEG)
        mask[kind] = jnp.concatenate([one] * groups, axis=1)
    copies.wait(0, n_kv)
    for i in range(kvbuf.shape[0] // block):
        here = pl.ds(i * block, block)
        vbuf[0:kv_cols, here] = kvbuf[here, kv_cols:].T
    copies.wait(n_kv)
    lane = lax.broadcasted_iota(jnp.int32, (block, kv_cols), 1)
    for i in range(n_steps):
        first = i * block
        q = qbuf[pl.ds(first, block)]
        k = kvbuf[pl.ds(first, span), :kv_cols]
        bias = mask[edges.index(i) + 1 if i in edges else 0]
        scores = []
        for g in range(kv_local):
            mine = (lane >= g * HD) & (lane < (g + 1) * HD)
            tiles = []
            for j in range(groups):
                tile = q[:, j * kv_cols : (j + 1) * kv_cols]
                tiles.append(jnp.where(mine, tile, jnp.zeros_like(tile)))
            scores.append(dot_t(k, jnp.concatenate(tiles, axis=0)))
        weights = []
        rests = []
        for g in range(kv_local):
            s = scores[g] + bias
            sink = jnp.concatenate(
                [jnp.full((1, block), sink_ref[g * groups + j], F32) for j in range(groups)], axis=1
            )
            top = jnp.maximum(jnp.max(s, axis=0, keepdims=True), sink)
            weights.append(jnp.exp(s - top).astype(BF16))
            rests.append(jnp.exp(sink - top))
        outs = []
        for g in range(kv_local):
            v = vbuf[g * HD : (g + 1) * HD, pl.ds(first, span)]
            ones = vbuf[kv_cols : kv_cols + 16, pl.ds(first, span)]
            o = dot(jnp.concatenate([v, ones], axis=0), weights[g])
            o = o[:HD] / (o[HD : HD + 1] + rests[g])
            outs += [o[:, j * block : (j + 1) * block] for j in range(groups)]
        out_ref[pl.ds(first, block)] = jnp.concatenate(outs, axis=0).T.astype(BF16)


def attend(sink, proj, low, high, kv_local, groups, seq_len, start, rows):
    n = len(proj)
    width = proj[0].shape[2]
    total = sum(p.shape[1] for p in proj)
    kv_cols = kv_local * HD
    return pl.pallas_call(
        functools.partial(attend_kernel, n, kv_local, groups, seq_len, total, start),
        out_shape=jax.ShapeDtypeStruct((rows, width), BF16),
        in_specs=[SMEM] + [HBM] * n + [VMEM, VMEM],
        out_specs=VMEM,
        scratch_shapes=[
            pltpu.VMEM((rows, width), BF16),
            pltpu.VMEM((rows + 2 * WINDOW, 2 * kv_cols), BF16),
            pltpu.VMEM((kv_cols + 16, rows + 2 * WINDOW), BF16),
            pltpu.VMEM((3, 3 * WINDOW, groups * WINDOW), F32),
            pltpu.SemaphoreType.DMA((2 * len(runs()),)),
        ],
        cost_estimate=cost(0.8e9, 3 << 20),
        compiler_params=PARAMS,
        name="attend",
    )(sink, *in_hbm(proj), low, high)


def totals_kernel(n_chunks, ret_local, n_sp, *refs):
    ccol_ref = refs[0]
    sum_refs = refs[1 : 1 + n_chunks]
    out_ref = refs[-1]
    me = lax.axis_index("sp")
    last = ccol_ref.shape[0] - 1
    line = lax.broadcasted_iota(jnp.int32, (EXTRA, RV), 0)
    for h in range(ret_local):
        sums = sum_refs[0][h]
        for ref in sum_refs[1:]:
            sums = sums + ref[h]
        end = jnp.broadcast_to(ccol_ref[last : last + 1, h : h + 1], (EXTRA, RV))
        d0 = end.astype(BF16).astype(F32)
        d1 = (end - d0).astype(BF16).astype(F32)
        d2 = end - d0 - d1
        extra = jnp.where(line == 0, d0, jnp.where(line == 1, d1, jnp.where(line == 2, d2, 0.0)))
        fwd = jnp.concatenate([sums[:, :RV], extra], axis=0).astype(BF16)
        bwd = jnp.concatenate([sums[:, RV:], extra], axis=0).astype(BF16)
        for j in range(n_sp):
            out_ref[j, h] = jnp.where(j > me, fwd, bwd)


def totals(ccol, sums, n_sp):
    ret_local = sums[0].shape[0]
    return pl.pallas_call(
        functools.partial(totals_kernel, len(sums), ret_local, n_sp),
        out_shape=jax.ShapeDtypeStruct((n_sp, ret_local, RK + EXTRA, RV), BF16),
        in_specs=[VMEM] * (1 + len(sums)),
        out_specs=VMEM,
        cost_estimate=cost(0.1e9, 1 << 20),
        compiler_params=PARAMS,
        name="totals",
    )(ccol, *sums)


def retain_kernel(n_chunks, ret_local, n_sp, *refs):
    ccol_hbm, crow_hbm, got_hbm, init_hbm = refs[:4]
    proj = refs[4 : 4 + n_chunks]
    outs = refs[4 + n_chunks : 4 + n_chunks + HALVES]
    states, got_ref, init_ref, ccol_ref, crow_ref, rbuf, vbuf, gbuf, sems = refs[-9:]
    me = lax.axis_index("sp")
    total = ccol_ref.shape[0]
    last = total - 1
    cols = ret_local * RK
    copies = Copies(sems)
    copies.start(got_hbm, got_ref)
    copies.start(init_hbm, init_ref)
    copies.start(ccol_hbm, ccol_ref)
    copies.start(crow_hbm, crow_ref)
    size = total // 8
    for group, buf in ((2, rbuf), (3, vbuf), (4, gbuf)):
        for c, inner, first, count in runs():
            src = proj[c].at[group, pl.ds(inner * size, count * size)]
            copies.start(src, buf.at[pl.ds(first * size, count * size)])
    copies.wait(0, 2)
    states[...] = jnp.zeros(states.shape, BF16)
    for h in range(ret_local):
        ends = []
        for j in range(n_sp):
            tail = got_ref[j, h, RK : RK + EXTRA, :].astype(F32)
            ends.append(jnp.sum(tail, axis=0, keepdims=True))
        for side, order in enumerate((range(n_sp - 1, -1, -1), range(n_sp))):
            state = jnp.zeros((RK, RV), F32)
            run = jnp.zeros((1, RV), F32)
            for j in order:
                here = (j < me) if side == 0 else (j > me)
                term = jnp.exp(run) * got_ref[j, h, 0:RK, :].astype(F32)
                state = state + jnp.where(here, term, 0.0)
                run = run + jnp.where(here, ends[j], 0.0)
            state = state + jnp.exp(run) * init_ref[side, h]
            col = (2 * h + side) * RV
            states[h * RK : (h + 1) * RK, col : col + RV] = state.astype(BF16)
    copies.wait(2)
    block = min(256, total // HALVES)
    lane = lax.broadcasted_iota(jnp.int32, (block, cols), 1)
    for i in range(total // block):
        here = pl.ds(i * block, block)
        out_ref = outs[i * block * HALVES // total]
        there = pl.ds(i * block % (total // HALVES), block)
        q = rbuf[here, :cols]
        both = dot(q, states[...])
        for h in range(ret_local):
            mine = (lane >= h * RK) & (lane < (h + 1) * RK)
            qh = jnp.where(mine, q, jnp.zeros_like(q))
            col = ccol_ref[here, h : h + 1]
            end = ccol_ref[last : last + 1, h : h + 1]
            gap = col - crow_ref[h : h + 1, :]
            w = (dot_t(qh, rbuf[:, cols:]) * jnp.exp(-jnp.abs(gap))).astype(BF16)
            ret = (
                dot(w, vbuf[:, h * RV : (h + 1) * RV])
                + jnp.exp(col) * both[:, 2 * h * RV : (2 * h + 1) * RV]
                + jnp.exp(end - col) * both[:, (2 * h + 1) * RV : (2 * h + 2) * RV]
            )
            centered = ret - jnp.mean(ret, axis=1, keepdims=True)
            scale = lax.rsqrt(jnp.mean(centered * centered, axis=1, keepdims=True) + NORM_EPS)
            gate = gbuf[here, h * RV : (h + 1) * RV].astype(F32)
            gated = gate / (1.0 + jnp.exp(-gate))
            out_ref[there, h * RV : (h + 1) * RV] = (gated * (centered * scale)).astype(BF16)


def retain(ccol, crow, got, init, proj, ret_local, n_sp):
    n = len(proj)
    width = proj[0].shape[2]
    total = ccol.shape[0]
    return pl.pallas_call(
        functools.partial(retain_kernel, n, ret_local, n_sp),
        out_shape=(jax.ShapeDtypeStruct((total // HALVES, width), BF16),) * HALVES,
        in_specs=[HBM] * (n + 4),
        out_specs=(VMEM,) * HALVES,
        scratch_shapes=[
            pltpu.VMEM((ret_local * RK, 2 * ret_local * RV), BF16),
            pltpu.VMEM(got.shape, BF16),
            pltpu.VMEM(init.shape, F32),
            pltpu.VMEM(ccol.shape, F32),
            pltpu.VMEM(crow.shape, F32),
            pltpu.VMEM((total, width), BF16),
            pltpu.VMEM((total, width), BF16),
            pltpu.VMEM((total, width), BF16),
            pltpu.SemaphoreType.DMA((3 * len(runs()) + 4,)),
        ],
        cost_estimate=cost(1.5e9, 4 << 20),
        compiler_params=PARAMS,
        name="retain",
    )(*in_hbm([ccol, crow, got, init, *proj]))


def most_kernel(n_far, n_data, *refs):
    near_att, near_ret, peer_att, peer_ret = refs[:4]
    far_att, far_ret = refs[4 : 4 + n_far], refs[4 + n_far : 4 + 2 * n_far]
    data = refs[4 + 2 * n_far : 4 + 2 * n_far + n_data]
    out_ref, rest_ref = refs[4 + 2 * n_far + n_data : 6 + 2 * n_far + n_data]
    left, right, sems = refs[-3:]
    copies = Copies(sems)
    cols = out_ref.shape[1]
    tp = lax.axis_index("tp")
    mine = pl.ds(pl.multiple_of(tp * cols, cols), cols)
    half = pl.ds(pl.multiple_of(lax.rem(tp, 2) * cols, cols), cols)
    depth = near_att.shape[0]
    rows = [(ref, mine) for ref in (near_att, peer_att)] + [(ref, half) for ref in far_att]
    rows += [(ref, mine) for ref in (near_ret, peer_ret)]
    for i, (ref, at) in enumerate(rows):
        copies.start(ref.at[:, at], right.at[pl.ds(i * depth, depth)])
    for i, ref in enumerate(data):
        half_rows = pl.ds(i % HALVES * ref.shape[0], ref.shape[0])
        copies.start(ref, left.at[half_rows, pl.ds(i // HALVES * depth, depth)])
    for i, ref in enumerate(far_ret):
        copies.start(ref.at[:, half], rest_ref.at[pl.ds(i * depth, depth)])
    copies.wait()
    rows = min(256, out_ref.shape[0])
    for i in range(out_ref.shape[0] // rows):
        here = pl.ds(i * rows, rows)
        out_ref[here] = dot(left[here], right[...])


def most(weights, data, cols):
    total, depth = data[0].shape[0] * HALVES, data[0].shape[1]
    n = len(data)
    n_far = (len(weights) - 4) // 2
    return pl.pallas_call(
        functools.partial(most_kernel, n_far, n),
        out_shape=(
            pltpu.VMEM((total, cols), F32),
            pltpu.VMEM((n_far * depth, cols), BF16),
        ),
        in_specs=[HBM] * (len(weights) + n),
        out_specs=(VMEM, VMEM),
        scratch_shapes=[
            pltpu.VMEM((total, n // HALVES * depth), BF16),
            pltpu.VMEM((n // HALVES * depth, cols), BF16),
            pltpu.SemaphoreType.DMA((len(weights) + n,)),
        ],
        cost_estimate=cost(1e9, 8 << 20),
        compiler_params=PARAMS,
        name="most",
    )(*in_hbm(weights), *in_hbm(data))


def last_kernel(n_data, start, *refs):
    base, right = refs[:2]
    data = refs[2 : 2 + n_data]
    out_ref, held, sems = refs[-3:]
    copies = Copies(sems)
    rows = held.shape[1]
    for i in range(held.shape[0]):
        here = pl.ds(i * rows, rows)
        there = pl.ds(start + i * rows, rows)
        part = dot(jnp.concatenate([ref[here] for ref in data], axis=1), right[...])
        held[i] = (part + base[there]).astype(BF16)
        copies.start(held.at[i], out_ref.at[there])
    copies.wait()


def last(base, right, data, start, done):
    total, cols = base.shape
    part = data[0].shape[0]
    rows = min(256, part)
    n = len(data)
    extra = [] if done is None else [done]
    return pl.pallas_call(
        functools.partial(last_kernel, n, start),
        out_shape=jax.ShapeDtypeStruct((total, cols), BF16),
        in_specs=[VMEM] * (2 + n) + [HBM] * len(extra),
        out_specs=HBM,
        scratch_shapes=[
            pltpu.VMEM((part // rows, rows, cols), BF16),
            pltpu.SemaphoreType.DMA((part // rows,)),
        ],
        input_output_aliases={} if done is None else {2 + n: 0},
        cost_estimate=cost(0.5e9, 4 << 20),
        compiler_params=PARAMS,
        name="last",
    )(*in_vmem([base, right]), *data, *extra)


def core_swap(value):
    n = lax.axis_size("tp")
    return lax.ppermute(value, "tp", [(i, i ^ 1) for i in range(n)])


def chip_turn(value, by):
    n = lax.axis_size("tp")
    return lax.ppermute(value, "tp", [(i, (i + 2 * by) % n) for i in range(n)])


def gather_tp(value):
    blocks = [value, core_swap(value)]
    for by in range(1, lax.axis_size("tp") // 2):
        far = chip_turn(value, by)
        blocks += [far, core_swap(far)]
    return blocks


def sources():
    n = lax.axis_size("tp")
    me = lax.axis_index("tp")
    out = [me, me ^ 1]
    for by in range(1, n // 2):
        far = lax.rem(me + (n - 2 * by), n)
        out += [far, far ^ 1]
    return out


def output_weights(out_att, out_ret, slabs):
    peers = [core_swap(w) for w in (out_att, out_ret)]
    att, ret = [], []
    for i, piece in enumerate(slabs):
        by = i // 2 + 1
        moved = chip_turn(piece, by)
        (att if i % 2 == 0 else ret).extend([moved, core_swap(moved)])
    return [out_att, out_ret] + peers + att + ret


def body(
    tokens,
    norm_gain,
    att_query,
    att_key,
    att_value,
    ret_query,
    ret_key,
    ret_value,
    ret_gate,
    att_sink,
    decay_log,
    init_state,
    out_att,
    out_ret,
):
    n_sp = lax.axis_size("sp")
    total = tokens.shape[0]
    seq_len = total * n_sp
    width = att_query.shape[1]
    half = width // 2
    kv_local = att_key.shape[1] // HD
    groups = att_sink.shape[0] // kv_local
    ret_local = decay_log.shape[0]
    cols = tokens.shape[1]

    slabs = slab(out_att, out_ret, cols)
    pieces = list(split(tokens, 0, 1))
    pieces += split(tokens, 1, len(CHUNKS))
    near = core_swap(tokens)
    far = {}
    for c in range(len(CHUNKS)):
        far[c] = []
        for by in range(1, lax.axis_size("tp") // 2):
            block = chip_turn(pieces[c], by)
            far[c] += [block, core_swap(block)]

    lane = np.arange(ret_local * RK)
    swap = np.zeros((lane.size, lane.size), np.float32)
    swap[lane ^ (RK // 2), lane] = np.where(lane % RK < RK // 2, -1.0, 1.0)
    swap = jnp.asarray(swap, BF16)
    mix = np.zeros((width, width), np.float32)
    for g in range(kv_local):
        for j in range(groups):
            for i in range(HD):
                mix[(g * groups + j) * HD + i, (j * kv_local + g) * HD + i] = 1.0
    mix = jnp.asarray(mix, BF16)

    if half % 128 == 0:
        weights = [att_query, att_key, att_value, ret_query, ret_key, ret_value, ret_gate]
        parts = [(0, 0), (1, 0), (1, half), (2, 0), (2, half), (3, 0), (4, 0)]
    else:
        weights = [
            att_query,
            jnp.concatenate([att_key, att_value], axis=1),
            jnp.concatenate([ret_query, ret_key], axis=1),
            ret_value,
            ret_gate,
        ]
        parts = [(i, 0) for i in range(5)]
    gain = norm_gain[None, :]
    weights = in_vmem(weights)
    crow, ccol, cos, sin = prepare(decay_log, [])
    out_w = output_weights(out_att, out_ret, slabs)
    proj = [None] * len(CHUNKS)
    sums = [None] * len(CHUNKS)
    edges = []
    for c, eighths in enumerate(CHUNKS):
        proj[c], sums[c], *found = project(
            gain, ccol, swap, mix, cos, sin, [tokens, near] + far[c], weights, parts,
            eighths, ret_local,
        )
        edges += found

    edge0 = lax.ppermute(edges[0], "sp", [(i, i ^ 1) for i in range(n_sp)])
    turn = [(i, (((i + 1) ^ 1) + n_sp - 1) % n_sp) for i in range(n_sp)]
    edge1 = lax.ppermute(edges[1], "sp", turn)
    sent = totals(ccol, sums, n_sp)
    got = lax.all_to_all(sent, "sp", 0, 0, tiled=True)
    part = total // HALVES
    att_blocks = []
    for i in range(HALVES):
        attended = attend(att_sink, proj, edge0, edge1, kv_local, groups, seq_len, i * part, part)
        att_blocks.append(gather_tp(attended))
    kept = retain(ccol, crow, got, init_state, proj, ret_local, n_sp)
    ret_blocks = [gather_tp(kept[i]) for i in range(HALVES)]
    att_pieces = [block for pair in zip(*att_blocks) for block in pair]
    ret_pieces = [block for pair in zip(*ret_blocks) for block in pair]
    base, right = most(out_w, att_pieces + ret_pieces[: 2 * HALVES], cols)
    done = None
    for i in range(HALVES):
        done = last(base, right, ret_blocks[i][2:], i * part, done)
    return done


def solution(mesh):
    in_specs = (
        P("sp", "tp"),
        P(),
        P(None, "tp"),
        P(None, "tp"),
        P(None, "tp"),
        P(None, "tp"),
        P(None, "tp"),
        P(None, "tp"),
        P(None, "tp"),
        P("tp"),
        P("tp", "sp"),
        P(None, "tp", None, None),
        P("tp", None),
        P("tp", None),
    )
    out_specs = P("sp", "tp")
    return jax.shard_map(body, mesh=mesh, in_specs=in_specs, out_specs=out_specs, check_vma=False)
```
